512 devices in a mesh: sp: 64 (over z, y), tp: 8 (over x, core).
Axes of the slice: x: 4, y: 4, z: 16, core: 2. Of those that a mesh axis runs over, the one named last changes fastest.
Arguments:
- latent: bfloat16 [16384, 2048], P(('sp', 'tp')), may hold values from -6 to 6
- condition: bfloat16 [2048], P('sp'), may hold values from -6 to 6
- context_condition: bfloat16 [2048], P('sp'), may hold values from -6 to 6
- context: bfloat16 [512, 2048], P('sp'), may hold values from -6 to 6
- w_shift: bfloat16 [2048, 2048], P('sp', 'tp'), may hold values from -0.125 to 0.125
- w_scale: bfloat16 [2048, 2048], P('sp', 'tp'), may hold values from -0.125 to 0.125
- w_gate: bfloat16 [2048, 2048], P('sp', 'tp'), may hold values from -0.125 to 0.125
- pre_gain: float32 [2048], replicated, may hold values from 0.1 to 1.9
- post_gain: float32 [2048], replicated, may hold values from 0.1 to 1.9
- query_gain: float32 [128], replicated, may hold values from 0.1 to 5
- key_gain: float32 [128], replicated, may hold values from 0.1 to 5
- w_query: bfloat16 [2048, 2048], P(None, 'tp'), may hold values from -0.125 to 0.125
- w_key: bfloat16 [2048, 1024], P(None, 'tp'), may hold values from -0.125 to 0.125
- w_value: bfloat16 [2048, 1024], P(None, 'tp'), may hold values from -0.125 to 0.125
- w_out: bfloat16 [2048, 2048], P('tp'), may hold values from -0.125 to 0.125
Outputs:
- updated: bfloat16 [16384, 2048], P(('sp', 'tp'))
The draws below stay inside these ranges and needn't reach their ends.
All inputs are finite; a program needn't handle non-finite values.
Results may differ from the reference program's by a relative error of at most 0.0085.
The reference program's roundings to bfloat16 on the way count: a program that leaves them out, or rounds other values in their place, can miss the bound.
Values may be sent and summed in bfloat16 or wider, within the bound.
No kernel may reach another device: no remote copies, remote signals or barrier semaphores. Data moves between devices by JAX's collectives and lax.ppermute only.
A program may use at most 64 MiB of HBM per device.

```python
import math
import jax
import jax.numpy as jnp
from jax import lax

D = 2048
HEADS = 16
KV_HEADS = 8
HEAD_DIM = 128
GRID_W = 64
CTX = 512
TOKENS = 16384
N_TP = 8


def gain_draw(key):
    return 1.0 + 0.18 * jnp.clip(jax.random.normal(key, (HEAD_DIM,), jnp.float32), -4.5, 4.5)


def draw_query_gain(key, part):
    return gain_draw(jax.random.fold_in(key, 11))


def draw_key_gain(key, part):
    return gain_draw(jax.random.fold_in(key, 23))


def block_scale(key, extent, cuts, smallest, top_value):
    factor_of = 1.0
    for position, parts in cuts:
        steps = jax.random.uniform(jax.random.fold_in(jax.random.fold_in(key, 6), position), (parts,), jnp.float32, smallest / len(cuts), top_value / len(cuts))
        factor_of = factor_of * jnp.repeat(jnp.exp(steps), extent[position] // parts).reshape((-1,) + (1,) * (len(extent) - 1 - position))
    return factor_of


def gaussian(key, extent, deviation, bound, cuts=(), held_as=jnp.bfloat16):
    level = block_scale(key, extent, cuts, -0.22, 0.18) if cuts else 1.0
    drawn = jax.random.normal(key, extent, jnp.float32) * deviation * level
    return jnp.minimum(jnp.maximum(drawn, -bound), bound).astype(held_as)


def setup_inputs(seed: int = 0) -> dict:
    arg_keys = jax.random.split(jax.random.key(seed), 16)
    return {
        "latent": gaussian(arg_keys[0], (TOKENS, D), 1.0, 6.0, ((0, 512),)),
        "condition": gaussian(arg_keys[1], (D,), 1.0, 6.0, ((0, 64),)),
        "context_condition": gaussian(arg_keys[2], (D,), 1.0, 6.0, ((0, 64),)),
        "context": gaussian(arg_keys[3], (CTX, D), 1.0, 6.0, ((0, 64),)),
        "w_shift": gaussian(arg_keys[4], (D, D), D ** -0.5, 0.125, ((0, 64), (1, 8))),
        "w_scale": gaussian(arg_keys[5], (D, D), D ** -0.5, 0.125, ((0, 64), (1, 8))),
        "w_gate": gaussian(arg_keys[6], (D, D), D ** -0.5, 0.125, ((0, 64), (1, 8))),
        "pre_gain": jnp.clip(1.0 + 0.18 * jax.random.normal(arg_keys[7], (D,), jnp.float32), 0.1, 1.9),
        "post_gain": jnp.clip(1.0 + 0.18 * jax.random.normal(arg_keys[8], (D,), jnp.float32), 0.1, 1.9),
        "query_gain": draw_query_gain(jax.random.fold_in(arg_keys[15], 71), 0),
        "key_gain": draw_key_gain(jax.random.fold_in(arg_keys[15], 71), 0),
        "w_query": gaussian(arg_keys[11], (D, HEADS * HEAD_DIM), D ** -0.5, 0.125, ((1, 8),)),
        "w_key": gaussian(arg_keys[12], (D, KV_HEADS * HEAD_DIM), D ** -0.5, 0.125, ((1, 8),)),
        "w_value": gaussian(arg_keys[13], (D, KV_HEADS * HEAD_DIM), D ** -0.5, 0.125, ((1, 8),)),
        "w_out": gaussian(arg_keys[14], (HEADS * HEAD_DIM, D), (HEADS * HEAD_DIM) ** -0.5, 0.125, ((0, 8),)),
    }


def rms(values, gain):
    values = values.astype(jnp.float32)
    return values * lax.rsqrt(lax.optimization_barrier(jnp.mean(values * values, axis=-1, keepdims=True)) + 1e-06) * gain

def rotate_grid(values, positions, grid_width):
    head_dim = values.shape[-1]
    half = head_dim // 2
    quarter = head_dim // 4
    freqs = 10000.0 ** (-jnp.arange(0, half, 2).astype(jnp.float32) / half)
    row_pos = (positions // grid_width).astype(jnp.float32)
    col_pos = (positions % grid_width).astype(jnp.float32)
    pieces = []
    for axis_pos, base in ((row_pos, 0), (col_pos, half)):
        angle = axis_pos[:, None, None] * freqs
        cosine = jnp.cos(angle)
        sine = jnp.sin(angle)
        first = values[..., base:base + quarter]
        second = values[..., base + quarter:base + half]
        pieces = pieces + [first * cosine - second * sine, second * cosine + first * sine]
    return jnp.concatenate(pieces, axis=-1)

def reference(latent, condition, context_condition, context, w_shift, w_scale, w_gate, pre_gain, post_gain, query_gain, key_gain, w_query, w_key, w_value, w_out):
    head_dim = HEAD_DIM
    group = HEADS // KV_HEADS
    conds = jax.nn.silu(jnp.stack([condition, context_condition]).astype(jnp.float32)).astype(jnp.bfloat16)
    shift = jnp.dot(conds, w_shift, preferred_element_type=jnp.float32)
    scale = jnp.dot(conds, w_scale, preferred_element_type=jnp.float32)
    gate = jnp.dot(conds, w_gate, preferred_element_type=jnp.float32)
    normed = (rms(latent, pre_gain) * (1.0 + scale[0]) + shift[0]).astype(jnp.bfloat16)
    normed_context = (rms(context, pre_gain) * (1.0 + scale[1]) + shift[1]).astype(jnp.bfloat16)
    positions = jnp.arange(TOKENS).astype(jnp.int32)
    query = jnp.dot(normed, w_query, preferred_element_type=jnp.float32).reshape(TOKENS, HEADS, head_dim)
    query = rotate_grid(rms(query, query_gain), positions, GRID_W).astype(jnp.bfloat16)
    key = jnp.dot(normed, w_key, preferred_element_type=jnp.float32).reshape(TOKENS, KV_HEADS, head_dim)
    key = rotate_grid(rms(key, key_gain), positions, GRID_W).astype(jnp.bfloat16)
    value = jnp.dot(normed, w_value, preferred_element_type=jnp.float32).astype(jnp.bfloat16)
    value = value.reshape(TOKENS, KV_HEADS, head_dim)
    context_key = jnp.dot(normed_context, w_key, preferred_element_type=jnp.float32).reshape(CTX, KV_HEADS, head_dim)
    context_key = rms(context_key, key_gain).astype(jnp.bfloat16)
    context_value = jnp.dot(normed_context, w_value, preferred_element_type=jnp.float32).astype(jnp.bfloat16)
    context_value = context_value.reshape(CTX, KV_HEADS, head_dim)
    all_keys = jnp.concatenate([key, context_key], axis=0).astype(jnp.float32)
    all_values = jnp.concatenate([value, context_value], axis=0).astype(jnp.float32)
    lift = math.log(TOKENS / (4.0 * CTX))
    offsets = jnp.concatenate([jnp.zeros((TOKENS,), jnp.float32), jnp.full((CTX,), lift, jnp.float32)])
    block = 128
    blocked = query.reshape(TOKENS // block, block, KV_HEADS, group, head_dim)

    def one_block(query_block):
        scores = jnp.einsum('tkgd,skd->kgts', query_block.astype(jnp.float32), all_keys) * head_dim ** (-0.5)
        scores = scores + offsets
        largest = lax.optimization_barrier(jnp.max(scores, axis=-1, keepdims=True))
        terms = jnp.exp(scores - largest)
        total = lax.optimization_barrier(jnp.sum(terms, axis=-1))
        rounded = lax.optimization_barrier(terms.astype(jnp.bfloat16)).astype(jnp.float32)
        summed = jnp.einsum('kgts,skd->kgtd', rounded, all_values)
        result = summed / total[..., None]
        return result.transpose(2, 0, 1, 3).reshape(block, HEADS * head_dim).astype(jnp.bfloat16)
    attended = lax.map(one_block, blocked).reshape(TOKENS, HEADS * head_dim)
    group_width = HEADS * head_dim // N_TP
    mixed = jnp.zeros((TOKENS, D), jnp.float32)
    for index in range(N_TP):
        columns = attended[:, index * group_width:(index + 1) * group_width]
        rows_out = w_out[index * group_width:(index + 1) * group_width]
        partial_value = jnp.dot(columns, rows_out, preferred_element_type=jnp.float32).astype(jnp.bfloat16)
        mixed = mixed + lax.optimization_barrier(partial_value).astype(jnp.float32)
    updated = latent.astype(jnp.float32) + gate[0] * rms(mixed, post_gain)
    return updated.astype(jnp.bfloat16)
```

```python
import functools
import math

import jax
import jax.numpy as jnp
from jax import lax
from jax.experimental import pallas as pl
from jax.experimental.pallas import tpu as pltpu
from jax.sharding import Mesh
from jax.sharding import PartitionSpec as P

GRID_W = 64
LOG2E = math.log2(math.e)
ALL = ("z", "y", "tp")
F32 = jnp.float32
BF16 = jnp.bfloat16

STAGES = [[(s, 1), (-s, -1)] for s in range(1, 8)] + [[(8, 1)]]


def from_everyone(value, axes):
    devices = lax.axis_size(axes)
    return lax.all_to_all(
        jnp.broadcast_to(value[None], (devices, *value.shape)), axes, 0, 0, tiled=True
    )


def rms_rows(values):
    return values * lax.rsqrt(jnp.mean(values * values, axis=-1, keepdims=True) + 1e-06)


def rms(values, gain):
    values = values.astype(F32)
    return rms_rows(values) * gain


def rotation_tables(positions, grid_width, head_dim):
    half = head_dim // 2
    quarter = head_dim // 4
    lane = jnp.arange(head_dim)
    j = (lane % quarter).astype(F32)
    freqs = 10000.0 ** (-(2.0 * j) / half)
    row_pos = (positions // grid_width).astype(F32)[:, None]
    col_pos = (positions % grid_width).astype(F32)[:, None]
    angle = jnp.where(lane[None] < half, row_pos, col_pos) * freqs[None]
    first = ((lane % half) < quarter)[None]
    sine = jnp.sin(angle)
    return (
        jnp.cos(angle),
        jnp.where(first, -sine, 0.0),
        jnp.where(first, 0.0, sine),
    )


def project_kernel(lat, ctx, gain, mods, wq, wk, wv, qg, kg, cos, sa, sb, q_out, msg):
    rows = lat.shape[0]
    ctx_rows = ctx.shape[0]
    head_dim = kg.shape[1]
    quarter = head_dim // 4
    g = gain[...]
    x = rms_rows(lat[...].astype(F32)) * g
    x = (x * (1.0 + mods[1:2]) + mods[0:1]).astype(BF16)
    c = rms_rows(ctx[...].astype(F32)) * g
    c = (c * (1.0 + mods[3:4]) + mods[2:3]).astype(BF16)

    def turned(v, gain_row):
        v = rms_rows(v) * gain_row
        up = pltpu.roll(v, head_dim - quarter, 1)
        down = pltpu.roll(v, quarter, 1)
        return v * cos[...] + up * sa[...] + down * sb[...]

    both = jnp.concatenate([x, c], axis=0)
    k = jnp.dot(both, wk[...], preferred_element_type=F32)
    v = jnp.dot(both, wv[...], preferred_element_type=F32)
    msg[0:rows] = turned(k[:rows], kg[...]).astype(BF16)
    msg[rows : 2 * rows] = v[:rows].astype(BF16)
    tail = jnp.concatenate([rms_rows(k[rows:]) * kg[...], v[rows:]], axis=0)
    msg[2 * rows : 2 * rows + 2 * ctx_rows] = tail.astype(BF16)
    q = jnp.dot(x, wq[...], preferred_element_type=F32)
    for h in range(q.shape[1] // head_dim):
        qh = turned(q[:, h * head_dim : (h + 1) * head_dim], qg[...])
        q_out[:, h * rows : (h + 1) * rows] = jnp.transpose(qh).astype(BF16)


def attend_kernel(*refs, blocks, keys, has_ctx, first, last, factor, lift):
    refs = list(refs)
    q = refs.pop(0)
    kv = [refs.pop(0) for _ in range(blocks)]
    ctx = refs.pop(0) if has_ctx else None
    if not first:
        m_in, l_in, acc_in = refs.pop(0), refs.pop(0), refs.pop(0)
    qv = q[0]
    scores = [jnp.dot(r[0:keys], qv, preferred_element_type=F32) for r in kv]
    largest = functools.reduce(jnp.maximum, [jnp.max(s, axis=0, keepdims=True) for s in scores])
    largest = largest * factor
    values = [r[keys : 2 * keys] for r in kv]
    if has_ctx:
        half = ctx.shape[0] // 2
        cs = jnp.dot(ctx[0:half], qv, preferred_element_type=F32) * factor + lift
        largest = jnp.maximum(largest, jnp.max(cs, axis=0, keepdims=True))
    if not first:
        largest = jnp.maximum(largest, m_in[0])
        fade = jnp.exp2(m_in[0] - largest)
        total = l_in[0] * fade
        acc = acc_in[0] * fade
    else:
        total = jnp.zeros_like(largest)
        acc = None
    terms = [jnp.exp2(s * factor - largest) for s in scores]
    if has_ctx:
        terms.append(jnp.exp2(cs - largest))
        values.append(ctx[half : 2 * half])
    for p, v in zip(terms, values):
        total = total + jnp.sum(p, axis=0, keepdims=True)
        part = lax.dot_general(
            v, p.astype(BF16), (((0,), (0,)), ((), ())), preferred_element_type=F32
        )
        acc = part if acc is None else acc + part
    if last:
        (out,) = refs
        dim = acc.shape[0]
        out[0, 0:dim] = (acc / total).astype(BF16)
        lse = largest + jnp.log2(total)
        hi = lse.astype(BF16).astype(F32)
        mid = (lse - hi).astype(BF16).astype(F32)
        low = lse - hi - mid
        row = lax.broadcasted_iota(jnp.int32, (16, lse.shape[1]), 0)
        packed = jnp.where(row == 0, hi, jnp.where(row == 1, mid, jnp.where(row == 2, low, 0.0)))
        out[0, dim : dim + 16] = packed.astype(BF16)
    else:
        m_out, l_out, acc_out = refs
        m_out[0] = largest
        l_out[0] = total
        acc_out[0] = acc


def attend(q_all, messages, ctx, carry, last, keys, factor, lift):
    parts, dim, width = q_all.shape
    first = carry is None
    full = lambda a: pl.BlockSpec(a.shape, lambda i: (0,) * a.ndim)
    part = lambda n: pl.BlockSpec((1, n, width), lambda i: (i, 0, 0))
    operands = [q_all, *messages]
    specs = [part(dim)] + [full(a) for a in messages]
    if ctx is not None:
        operands.append(ctx)
        specs.append(full(ctx))
    if not first:
        operands += list(carry)
        specs += [part(1), part(1), part(dim)]
    if last:
        out_shape = (jax.ShapeDtypeStruct((parts, dim + 16, width), BF16),)
        out_specs = (part(dim + 16),)
    else:
        out_shape = (
            jax.ShapeDtypeStruct((parts, 1, width), F32),
            jax.ShapeDtypeStruct((parts, 1, width), F32),
            jax.ShapeDtypeStruct((parts, dim, width), F32),
        )
        out_specs = (part(1), part(1), part(dim))
    all_keys = keys * len(messages) + (0 if ctx is None else ctx.shape[0] // 2)
    return pl.pallas_call(
        functools.partial(
            attend_kernel,
            blocks=len(messages),
            keys=keys,
            has_ctx=ctx is not None,
            first=first,
            last=last,
            factor=factor,
            lift=lift,
        ),
        grid=(parts,),
        in_specs=specs,
        out_specs=out_specs,
        out_shape=out_shape,
        cost_estimate=pl.CostEstimate(
            flops=4 * all_keys * parts * width * dim,
            bytes_accessed=2 * parts * width * dim * 4,
            transcendentals=all_keys * parts * width,
        ),
        name="attend",
    )(*operands)


def merge_kernel(parts, w_out, out):
    count, rows, width = parts.shape
    dim = rows - 16
    tail = [parts[i, dim : dim + 16].astype(F32) for i in range(count)]
    lse = [t[0:1] + t[1:2] + t[2:3] for t in tail]
    top = functools.reduce(jnp.maximum, lse)
    share = [jnp.exp2(v - top) for v in lse]
    whole = functools.reduce(jnp.add, share)
    merged = functools.reduce(
        jnp.add, [parts[i, 0:dim].astype(F32) * share[i] for i in range(count)]
    )
    merged = (merged / whole).astype(BF16)
    heads = w_out.shape[0] // dim
    rows = width // heads
    stacked = jnp.concatenate(
        [merged[:, h * rows : (h + 1) * rows] for h in range(heads)], axis=0
    )
    out[...] = lax.dot_general(
        stacked, w_out[...], (((0,), (0,)), ((), ())), preferred_element_type=F32
    ).astype(BF16)


def body(
    latent,
    condition,
    context_condition,
    context,
    w_shift,
    w_scale,
    w_gate,
    pre_gain,
    post_gain,
    query_gain,
    key_gain,
    w_query,
    w_key,
    w_value,
    w_out,
):
    tp_count = lax.axis_size("tp")
    z_count = lax.axis_size("z")
    y_count = lax.axis_size("y")
    model = latent.shape[1]
    head_dim = query_gain.shape[0]
    tok_dev = latent.shape[0] * tp_count
    ctx_dev = context.shape[0]
    heads_dev = w_query.shape[1] // head_dim
    factor = head_dim ** (-0.5) * LOG2E
    lift = math.log(tok_dev / (4.0 * ctx_dev)) * LOG2E

    gathered = from_everyone(latent, "tp").reshape(tok_dev, model)

    conds = jax.nn.silu(jnp.stack([condition, context_condition]).astype(F32)).astype(BF16)
    shift_part, scale_part, gate_part = (
        jnp.dot(conds, weight, preferred_element_type=F32) for weight in (w_shift, w_scale, w_gate)
    )
    partial_mod = jnp.concatenate(
        [shift_part[0:1], scale_part[0:1], shift_part[1:2], scale_part[1:2], gate_part[0:1]], axis=0
    )
    partial_mod = from_everyone(partial_mod, "z").sum(axis=0)
    pieces = from_everyone(partial_mod, ("y", "tp"))
    mods = pieces.reshape(y_count, tp_count, *partial_mod.shape).sum(axis=0)
    mods = mods.transpose(1, 0, 2).reshape(partial_mod.shape[0], model)

    positions = (lax.axis_index("z") * y_count + lax.axis_index("y")) * tok_dev + jnp.arange(tok_dev)
    cos, sa, sb = rotation_tables(positions, GRID_W, head_dim)
    msg_rows = 2 * tok_dev + 2 * ctx_dev
    query, message = pl.pallas_call(
        project_kernel,
        out_shape=(
            jax.ShapeDtypeStruct((head_dim, heads_dev * tok_dev), BF16),
            jax.ShapeDtypeStruct((msg_rows, head_dim), BF16),
        ),
        cost_estimate=pl.CostEstimate(
            flops=2 * tok_dev * model * 4 * head_dim,
            bytes_accessed=2 * model * (4 * head_dim + tok_dev),
            transcendentals=0,
        ),
        name="project",
    )(
        gathered,
        context,
        pre_gain[None],
        mods[0:4],
        w_query,
        w_key,
        w_value,
        query_gain[None],
        key_gain[None],
        cos,
        sa,
        sb,
    )

    def receive(value, hop):
        turn = [((i + hop) % z_count, i) for i in range(z_count)]
        return lax.ppermute(value, "z", turn)

    q_all = from_everyone(query, "y")
    held = {0: message}
    carry = None
    waiting = [message]
    for stage in STAGES:
        arrived = {d: receive(held[d - hop], hop) for d, hop in stage}
        carry = attend(q_all, waiting, None, carry, False, tok_dev, factor, lift)
        held.update(arrived)
        waiting = list(arrived.values())
    tails = [held[d][2 * tok_dev :] for d in sorted(held)]
    ctx = jnp.concatenate([t[:ctx_dev] for t in tails] + [t[ctx_dev:] for t in tails], axis=0)
    (partials,) = attend(q_all, waiting, ctx, carry, True, tok_dev, factor, lift)
    returned = lax.all_to_all(partials, "y", 0, 0, tiled=True)
    mixed = pl.pallas_call(
        merge_kernel,
        out_shape=jax.ShapeDtypeStruct((tok_dev, model), BF16),
        cost_estimate=pl.CostEstimate(
            flops=2 * tok_dev * model * heads_dev * head_dim,
            bytes_accessed=4 * tok_dev * model,
            transcendentals=0,
        ),
        name="merge",
    )(returned, w_out)
    arrived = lax.all_to_all(mixed.reshape(tp_count, -1, model), "tp", 0, 0, tiled=True)
    mixed = arrived.astype(F32).sum(axis=0)
    updated = latent.astype(F32) + mods[4] * rms(mixed, post_gain)
    return updated.astype(BF16)


def solution(mesh):
    tp_count = mesh.shape["tp"]
    torus = Mesh(mesh.devices.reshape(16, 4, tp_count), ALL)
    sp = ("z", "y")
    placed = (
        P(ALL, None),
        P(sp),
        P(sp),
        P(sp, None),
        P(sp, "tp"),
        P(sp, "tp"),
        P(sp, "tp"),
        P(),
        P(),
        P(),
        P(),
        P(None, "tp"),
        P(None, "tp"),
        P(None, "tp"),
        P("tp", None),
    )
    return jax.shard_map(
        body, mesh=torus, in_specs=placed, out_specs=P(ALL, None), check_vma=False
    )
```

```python
import functools
import math

import jax
import jax.numpy as jnp
from jax import lax
from jax.experimental import pallas as pl
from jax.experimental.pallas import tpu as pltpu
from jax.sharding import Mesh
from jax.sharding import PartitionSpec as P

GRID_W = 64
LOG2E = math.log2(math.e)
TP = ("x", "c")
ALL = ("z", "y", *TP)
F32 = jnp.float32
BF16 = jnp.bfloat16


def from_everyone(value, axes):
    devices = lax.axis_size(axes)
    return lax.all_to_all(
        jnp.broadcast_to(value[None], (devices, *value.shape)), axes, 0, 0, tiled=True
    )


def rms_rows(values):
    return values * lax.rsqrt(jnp.mean(values * values, axis=-1, keepdims=True) + 1e-06)


def rms(values, gain):
    values = values.astype(F32)
    return rms_rows(values) * gain


def rotation_tables(positions, grid_width, head_dim):
    half = head_dim // 2
    quarter = head_dim // 4
    lane = jnp.arange(head_dim)
    j = (lane % quarter).astype(F32)
    freqs = 10000.0 ** (-(2.0 * j) / half)
    row_pos = (positions // grid_width).astype(F32)[:, None]
    col_pos = (positions % grid_width).astype(F32)[:, None]
    angle = jnp.where(lane[None] < half, row_pos, col_pos) * freqs[None]
    first = ((lane % half) < quarter)[None]
    sine = jnp.sin(angle)
    return (
        jnp.cos(angle),
        jnp.where(first, -sine, 0.0),
        jnp.where(first, 0.0, sine),
    )


def project_kernel(place, *refs):
    mine, other = refs[:4], refs[4]
    ctx, gain, mods, wq, wk, wv, qg, kg, cos, sa, sb, q_out, msg, lat = refs[5:]
    rows = lat.shape[0]
    part = mine[0].shape[0]
    for h in range(4):
        at = jax.lax.rem(place[0] + h, 4) * 2
        lat[pl.ds(pl.multiple_of((at + place[1]) * part, part), part)] = mine[h][...]
        lat[pl.ds(pl.multiple_of((at + 1 - place[1]) * part, part), part)] = other[
            h * part : (h + 1) * part
        ]
    ctx_rows = ctx.shape[0]
    head_dim = kg.shape[1]
    quarter = head_dim // 4
    g = gain[...]
    x = rms_rows(lat[...].astype(F32)) * g
    x = (x * (1.0 + mods[1:2]) + mods[0:1]).astype(BF16)
    c = rms_rows(ctx[...].astype(F32)) * g
    c = (c * (1.0 + mods[3:4]) + mods[2:3]).astype(BF16)

    def turned(v, gain_row):
        v = rms_rows(v) * gain_row
        up = pltpu.roll(v, head_dim - quarter, 1)
        down = pltpu.roll(v, quarter, 1)
        return v * cos[...] + up * sa[...] + down * sb[...]

    both = jnp.concatenate([x, c], axis=0)
    k = jnp.dot(both, wk[...], preferred_element_type=F32)
    v = jnp.dot(both, wv[...], preferred_element_type=F32)
    msg[0:rows] = turned(k[:rows], kg[...]).astype(BF16)
    msg[rows : 2 * rows] = v[:rows].astype(BF16)
    tail = jnp.concatenate([rms_rows(k[rows:]) * kg[...], v[rows:]], axis=0)
    msg[2 * rows : 2 * rows + 2 * ctx_rows] = tail.astype(BF16)
    q = jnp.dot(x, wq[...], preferred_element_type=F32)
    for h in range(q.shape[1] // head_dim):
        qh = turned(q[:, h * head_dim : (h + 1) * head_dim], qg[...])
        qt = jnp.transpose(qh).astype(BF16)
        for i in range(q_out.shape[0]):
            q_out[i, :, h * rows : (h + 1) * rows] = qt


def attend_kernel(*refs, counts, keys, extra, first, last, factor, lift):
    refs = list(refs)
    q = refs.pop(0)
    span = 2 * (keys + extra)
    blocks = []
    for count in counts:
        ref = refs.pop(0)
        blocks += [(ref, i * span) for i in range(count)]
    if not first:
        m_in, l_in, acc_in = refs.pop(0), refs.pop(0), refs.pop(0)
    tails = [ref[at + 2 * keys : at + span].astype(F32) for ref, at in blocks]
    ctx_key = jnp.concatenate([t[:extra] for t in tails], axis=0).astype(BF16)
    ctx_value = jnp.concatenate([t[extra:] for t in tails], axis=0).astype(BF16)

    def tile(i, unused):
        qv = q[i]
        scores = [
            jnp.dot(ref[at : at + keys], qv, preferred_element_type=F32) for ref, at in blocks
        ]
        largest = functools.reduce(
            jnp.maximum, [jnp.max(s, axis=0, keepdims=True) for s in scores]
        )
        ctx_scores = jnp.dot(ctx_key, qv, preferred_element_type=F32) * factor + lift
        largest = jnp.maximum(largest * factor, jnp.max(ctx_scores, axis=0, keepdims=True))
        if not first:
            largest = jnp.maximum(largest, m_in[i])
        terms = jnp.exp2(ctx_scores - largest)
        total = jnp.sum(terms, axis=0, keepdims=True)
        acc = weighted(ctx_value, terms)
        if not first:
            fade = jnp.exp2(m_in[i] - largest)
            total = total + l_in[i] * fade
            acc = acc + acc_in[i] * fade
        for s, (ref, at) in zip(scores, blocks):
            terms = jnp.exp2(s * factor - largest)
            total = total + jnp.sum(terms, axis=0, keepdims=True)
            acc = acc + weighted(ref[at + keys : at + 2 * keys], terms)
        if last:
            (out,) = refs
            dim = acc.shape[0]
            out[i, 0:dim] = (acc / total).astype(BF16)
            lse = largest + jnp.log2(total)
            hi = lse.astype(BF16).astype(F32)
            mid = (lse - hi).astype(BF16).astype(F32)
            low = lse - hi - mid
            row = lax.broadcasted_iota(jnp.int32, (16, lse.shape[1]), 0)
            packed = jnp.where(
                row == 0, hi, jnp.where(row == 1, mid, jnp.where(row == 2, low, 0.0))
            )
            out[i, dim : dim + 16] = packed.astype(BF16)
        else:
            m_out, l_out, acc_out = refs
            m_out[i] = largest
            l_out[i] = total
            acc_out[i] = acc
        return unused

    lax.fori_loop(0, q.shape[0], tile, 0)


def weighted(values, terms):
    return lax.dot_general(
        values, terms.astype(BF16), (((0,), (0,)), ((), ())), preferred_element_type=F32
    )


def attend(q_all, bundles, carry, last, keys, extra, factor, lift):
    parts, dim, width = q_all.shape
    first = carry is None
    counts = tuple(b.shape[0] // (2 * (keys + extra)) for b in bundles)
    operands = [q_all, *bundles] + ([] if first else list(carry))
    if last:
        out_shape = (jax.ShapeDtypeStruct((parts, dim + 16, width), BF16),)
    else:
        out_shape = (
            jax.ShapeDtypeStruct((parts, 1, width), F32),
            jax.ShapeDtypeStruct((parts, 1, width), F32),
            jax.ShapeDtypeStruct((parts, dim, width), F32),
        )
    whole = pl.BlockSpec(memory_space=pltpu.VMEM)
    all_keys = (keys + extra) * sum(counts)
    return pl.pallas_call(
        functools.partial(
            attend_kernel,
            counts=counts,
            keys=keys,
            extra=extra,
            first=first,
            last=last,
            factor=factor,
            lift=lift,
        ),
        in_specs=[whole] * len(operands),
        out_specs=tuple([whole] * len(out_shape)),
        out_shape=out_shape,
        cost_estimate=pl.CostEstimate(
            flops=4 * all_keys * parts * width * dim,
            bytes_accessed=2 * parts * width * dim * 4,
            transcendentals=all_keys * parts * width,
        ),
        name="attend",
    )(*operands)


def merge_kernel(parts, w_out, out):
    count, rows, width = parts.shape
    dim = rows - 16
    tail = [parts[i, dim : dim + 16].astype(F32) for i in range(count)]
    lse = [t[0:1] + t[1:2] + t[2:3] for t in tail]
    top = functools.reduce(jnp.maximum, lse)
    share = [jnp.exp2(v - top) for v in lse]
    whole = functools.reduce(jnp.add, share)
    merged = functools.reduce(
        jnp.add, [parts[i, 0:dim].astype(F32) * share[i] for i in range(count)]
    )
    merged = (merged / whole).astype(BF16)
    heads = w_out.shape[0] // dim
    rows = width // heads
    stacked = jnp.concatenate(
        [merged[:, h * rows : (h + 1) * rows] for h in range(heads)], axis=0
    )
    out[...] = lax.dot_general(
        stacked, w_out[...], (((0,), (0,)), ((), ())), preferred_element_type=F32
    ).astype(BF16)


def body(
    latent,
    condition,
    context_condition,
    context,
    w_shift,
    w_scale,
    w_gate,
    pre_gain,
    post_gain,
    query_gain,
    key_gain,
    w_query,
    w_key,
    w_value,
    w_out,
):
    tp_count = lax.axis_size(TP)
    y_count = lax.axis_size("y")
    model = latent.shape[1]
    head_dim = query_gain.shape[0]
    tok_dev = latent.shape[0] * tp_count
    ctx_dev = context.shape[0]
    heads_dev = w_query.shape[1] // head_dim
    factor = head_dim ** (-0.5) * LOG2E
    lift = math.log(tok_dev / (4.0 * ctx_dev)) * LOG2E

    def receive(value, axis, hop):
        size = lax.axis_size(axis)
        return lax.ppermute(value, axis, [((i + hop) % size, i) for i in range(size)])

    mine = [latent] + [receive(latent, "x", h) for h in (1, 2, 3)]
    other = receive(jnp.concatenate(mine, axis=0), "c", 1)

    conds = jax.nn.silu(jnp.stack([condition, context_condition]).astype(F32)).astype(BF16)
    shift_part, scale_part, gate_part = (
        jnp.dot(conds, weight, preferred_element_type=F32) for weight in (w_shift, w_scale, w_gate)
    )
    partial_mod = jnp.concatenate(
        [shift_part[0:1], scale_part[0:1], shift_part[1:2], scale_part[1:2], gate_part[0:1]], axis=0
    )
    partial_mod = from_everyone(partial_mod, "z")
    partial_mod = partial_mod.sum(axis=0)
    pieces = from_everyone(partial_mod, ("y", *TP))
    mods = pieces.reshape(y_count, tp_count, *partial_mod.shape).sum(axis=0)
    mods = mods.transpose(1, 0, 2).reshape(partial_mod.shape[0], model)

    positions = (lax.axis_index("z") * y_count + lax.axis_index("y")) * tok_dev + jnp.arange(tok_dev)
    cos, sa, sb = rotation_tables(positions, GRID_W, head_dim)
    msg_rows = 2 * tok_dev + 2 * ctx_dev
    whole = pl.BlockSpec(memory_space=pltpu.VMEM)
    place = jnp.stack([lax.axis_index("x"), lax.axis_index("c")]).astype(jnp.int32)
    query, message = pl.pallas_call(
        project_kernel,
        in_specs=[pl.BlockSpec(memory_space=pltpu.SMEM)] + [whole] * 16,
        out_specs=(whole, whole),
        scratch_shapes=[pltpu.VMEM((tok_dev, model), BF16)],
        out_shape=(
            jax.ShapeDtypeStruct((y_count, head_dim, heads_dev * tok_dev), BF16),
            jax.ShapeDtypeStruct((msg_rows, head_dim), BF16),
        ),
        cost_estimate=pl.CostEstimate(
            flops=2 * tok_dev * model * 4 * head_dim,
            bytes_accessed=2 * model * (4 * head_dim + tok_dev),
            transcendentals=0,
        ),
        name="project",
    )(
        place,
        *mine,
        other,
        context,
        pre_gain[None],
        mods[0:4],
        w_query,
        w_key,
        w_value,
        query_gain[None],
        key_gain[None],
        cos,
        sa,
        sb,
    )

    far_up, far_down = receive(message, "z", 5), receive(message, "z", -5)
    up, down = receive(message, "z", 1), receive(message, "z", -1)
    q_all = lax.all_to_all(query, "y", 0, 0, tiled=True)
    ups = receive(jnp.concatenate([up, far_up, far_down], axis=0), "z", 1)
    downs = receive(jnp.concatenate([down, far_down, far_up], axis=0), "z", -1)
    opposite = receive(far_up, "z", 3)
    last_ups = receive(ups[: 2 * msg_rows], "z", 1)
    last_downs = receive(downs[: 2 * msg_rows], "z", -1)
    shared = (tok_dev, ctx_dev, factor, lift)
    carry = attend(q_all, [message, up, down, far_up, far_down], None, False, *shared)
    carry = attend(q_all, [ups, downs], carry, False, *shared)
    (partials,) = attend(q_all, [opposite, last_ups, last_downs], carry, True, *shared)
    returned = lax.all_to_all(partials, "y", 0, 0, tiled=True)
    mixed = pl.pallas_call(
        merge_kernel,
        out_shape=jax.ShapeDtypeStruct((tok_dev, model), BF16),
        cost_estimate=pl.CostEstimate(
            flops=2 * tok_dev * model * heads_dev * head_dim,
            bytes_accessed=4 * tok_dev * model,
            transcendentals=0,
        ),
        name="merge",
    )(returned, w_out)
    arrived = lax.all_to_all(mixed.reshape(tp_count, -1, model), TP, 0, 0, tiled=True)
    mixed = arrived.astype(F32).sum(axis=0)
    updated = latent.astype(F32) + mods[4] * rms(mixed, post_gain)
    return updated.astype(BF16)


def solution(mesh):
    torus = Mesh(mesh.devices.reshape(16, 4, 4, 2), ALL)
    sp = ("z", "y")
    placed = (
        P(ALL, None),
        P(sp),
        P(sp),
        P(sp, None),
        P(sp, TP),
        P(sp, TP),
        P(sp, TP),
        P(),
        P(),
        P(),
        P(),
        P(None, TP),
        P(None, TP),
        P(None, TP),
        P(TP, None),
    )
    return jax.shard_map(body, mesh=torus, in_specs=placed, out_specs=P(ALL, None), check_vma=False)
```

```python
import functools
import math

import jax
import jax.numpy as jnp
from jax import lax
from jax.experimental import pallas as pl
from jax.experimental.pallas import tpu as pltpu
from jax.sharding import Mesh
from jax.sharding import PartitionSpec as P

GRID_W = 64
LOG2E = math.log2(math.e)
TP = ("x", "c")
ALL = ("z", "y", *TP)
F32 = jnp.float32
BF16 = jnp.bfloat16


def room(mebibytes):
    return pltpu.CompilerParams(vmem_limit_bytes=mebibytes << 20)


def near(*arrays):
    return [pltpu.with_memory_space_constraint(a, pltpu.VMEM) for a in arrays]


def from_everyone(value, axes):
    devices = lax.axis_size(axes)
    return lax.all_to_all(
        jnp.broadcast_to(value[None], (devices, *value.shape)), axes, 0, 0, tiled=True
    )


def rms_rows(values):
    return values * lax.rsqrt(jnp.mean(values * values, axis=-1, keepdims=True) + 1e-06)


def rms(values, gain):
    values = values.astype(F32)
    return rms_rows(values) * gain


def rotation_tables(positions, grid_width, head_dim):
    half = head_dim // 2
    quarter = head_dim // 4
    lane = jnp.arange(head_dim)
    j = (lane % quarter).astype(F32)
    freqs = 10000.0 ** (-(2.0 * j) / half)
    row_pos = (positions // grid_width).astype(F32)[:, None]
    col_pos = (positions % grid_width).astype(F32)[:, None]
    angle = jnp.where(lane[None] < half, row_pos, col_pos) * freqs[None]
    first = ((lane % half) < quarter)[None]
    sine = jnp.sin(angle)
    return (
        jnp.cos(angle),
        jnp.where(first, -sine, 0.0),
        jnp.where(first, 0.0, sine),
    )


def modulation_kernel(cond, ctx_cond, w_shift, w_scale, w_gate, out):
    both = jnp.concatenate([cond[...].astype(F32), ctx_cond[...].astype(F32)], axis=0)
    both = jax.nn.silu(both).astype(BF16)
    shift, scale, gate = (
        jnp.dot(both, w[...], preferred_element_type=F32) for w in (w_shift, w_scale, w_gate)
    )
    rows = jnp.concatenate([shift[0:1], scale[0:1], shift[1:2], scale[1:2], gate[0:1]], axis=0)
    for i in range(out.shape[0]):
        out[i] = rows


def turned(v, gain_row, cos, sa, sb):
    head_dim = v.shape[1]
    quarter = head_dim // 4
    v = rms_rows(v) * gain_row
    up = pltpu.roll(v, head_dim - quarter, 1)
    down = pltpu.roll(v, quarter, 1)
    return v * cos[...] + up * sa[...] + down * sb[...]


def project_kernel(place, *refs):
    mine, other = refs[:4], refs[4]
    pieces, ctx, gain, wk, wv, kg, cos, sa, sb, msg, normed, gate, lat = refs[5:]
    rows = lat.shape[0]
    part = mine[0].shape[0]
    for h in range(4):
        at = jax.lax.rem(place[0] + h, 4) * 2
        lat[pl.ds(pl.multiple_of((at + place[1]) * part, part), part)] = mine[h][...]
        lat[pl.ds(pl.multiple_of((at + 1 - place[1]) * part, part), part)] = other[
            h * part : (h + 1) * part
        ]
    slots = 2 * 4
    mods = jnp.concatenate(
        [
            functools.reduce(
                jnp.add, [pieces[y * slots + t] for y in range(pieces.shape[0] // slots)]
            )
            for t in range(slots)
        ],
        axis=1,
    )
    gate[...] = mods[4:5]
    ctx_rows = ctx.shape[0]
    g = gain[...]
    x = rms_rows(lat[...].astype(F32)) * g
    x = (x * (1.0 + mods[1:2]) + mods[0:1]).astype(BF16)
    normed[...] = x
    c = rms_rows(ctx[...].astype(F32)) * g
    c = (c * (1.0 + mods[3:4]) + mods[2:3]).astype(BF16)
    both = jnp.concatenate([x, c], axis=0)
    k = jnp.dot(both, wk[...], preferred_element_type=F32)
    v = jnp.dot(both, wv[...], preferred_element_type=F32)
    msg[0:rows] = turned(k[:rows], kg[...], cos, sa, sb).astype(BF16)
    msg[rows : 2 * rows] = v[:rows].astype(BF16)
    tail = jnp.concatenate([rms_rows(k[rows:]) * kg[...], v[rows:]], axis=0)
    msg[2 * rows : 2 * rows + 2 * ctx_rows] = tail.astype(BF16)


def query_kernel(normed, wq, qg, cos, sa, sb, q_out):
    rows = normed.shape[0]
    head_dim = qg.shape[1]
    q = jnp.dot(normed[...], wq[...], preferred_element_type=F32)
    for h in range(q.shape[1] // head_dim):
        qh = turned(q[:, h * head_dim : (h + 1) * head_dim], qg[...], cos, sa, sb)
        qt = jnp.transpose(qh).astype(BF16)
        for i in range(q_out.shape[0]):
            q_out[i, :, h * rows : (h + 1) * rows] = qt


def attend_kernel(*refs, counts, keys, extra, first, last, factor, lift):
    refs = list(refs)
    q = refs.pop(0)
    span = 2 * (keys + extra)
    blocks = []
    for count in counts:
        ref = refs.pop(0)
        blocks += [(ref, i * span) for i in range(count)]
    if not first:
        m_in, l_in, acc_in = refs.pop(0), refs.pop(0), refs.pop(0)
    tails = [ref[at + 2 * keys : at + span].astype(F32) for ref, at in blocks]
    ctx_key = jnp.concatenate([t[:extra] for t in tails], axis=0).astype(BF16)
    ctx_value = jnp.concatenate([t[extra:] for t in tails], axis=0).astype(BF16)

    wide = 2
    width = q.shape[2]

    def both(ref, i):
        return jnp.concatenate([ref[wide * i + w] for w in range(wide)], axis=1)

    def tile(i, unused):
        qv = both(q, i)
        scores = [
            jnp.dot(ref[at : at + keys], qv, preferred_element_type=F32) for ref, at in blocks
        ]
        largest = functools.reduce(
            jnp.maximum, [jnp.max(s, axis=0, keepdims=True) for s in scores]
        )
        ctx_scores = jnp.dot(ctx_key, qv, preferred_element_type=F32) * factor + lift
        largest = jnp.maximum(largest * factor, jnp.max(ctx_scores, axis=0, keepdims=True))
        if not first:
            before = both(m_in, i)
            largest = jnp.maximum(largest, before)
        terms = jnp.exp2(ctx_scores - largest)
        total = jnp.sum(terms, axis=0, keepdims=True)
        acc = weighted(ctx_value, terms)
        if not first:
            fade = jnp.exp2(before - largest)
            total = total + both(l_in, i) * fade
            acc = acc + both(acc_in, i) * fade
        for s, (ref, at) in zip(scores, blocks):
            terms = jnp.exp2(s * factor - largest)
            total = total + jnp.sum(terms, axis=0, keepdims=True)
            acc = acc + weighted(ref[at + keys : at + 2 * keys], terms)
        if last:
            acc = acc / total
            lse = largest + jnp.log2(total)
            hi = lse.astype(BF16).astype(F32)
            mid = (lse - hi).astype(BF16).astype(F32)
            low = lse - hi - mid
            row = lax.broadcasted_iota(jnp.int32, (16, lse.shape[1]), 0)
            packed = jnp.where(
                row == 0, hi, jnp.where(row == 1, mid, jnp.where(row == 2, low, 0.0))
            )
        for w in range(wide):
            at = slice(w * width, (w + 1) * width)
            if last:
                (out,) = refs
                dim = acc.shape[0]
                out[wide * i + w, 0:dim] = acc[:, at].astype(BF16)
                out[wide * i + w, dim : dim + 16] = packed[:, at].astype(BF16)
            else:
                m_out, l_out, acc_out = refs
                m_out[wide * i + w] = largest[:, at]
                l_out[wide * i + w] = total[:, at]
                acc_out[wide * i + w] = acc[:, at]
        return unused

    lax.fori_loop(0, q.shape[0] // wide, tile, 0, unroll=True)


def weighted(values, terms):
    return lax.dot_general(
        values, terms.astype(BF16), (((0,), (0,)), ((), ())), preferred_element_type=F32
    )


def attend(q_all, bundles, carry, last, keys, extra, factor, lift):
    parts, dim, width = q_all.shape
    first = carry is None
    counts = tuple(b.shape[0] // (2 * (keys + extra)) for b in bundles)
    operands = [q_all, *bundles] + ([] if first else list(carry))
    if last:
        out_shape = (jax.ShapeDtypeStruct((parts, dim + 16, width), BF16),)
    else:
        out_shape = (
            pltpu.VMEM((parts, 1, width), F32),
            pltpu.VMEM((parts, 1, width), F32),
            pltpu.VMEM((parts, dim, width), F32),
        )
    whole = pl.BlockSpec(memory_space=pltpu.VMEM)
    all_keys = (keys + extra) * sum(counts)
    return pl.pallas_call(
        functools.partial(
            attend_kernel,
            counts=counts,
            keys=keys,
            extra=extra,
            first=first,
            last=last,
            factor=factor,
            lift=lift,
        ),
        in_specs=[whole] * len(operands),
        out_specs=tuple([whole] * len(out_shape)),
        out_shape=out_shape,
        cost_estimate=pl.CostEstimate(
            flops=4 * all_keys * parts * width * dim,
            bytes_accessed=2 * parts * width * dim * 4,
            transcendentals=all_keys * parts * width,
        ),
        compiler_params=room(32),
        name="attend",
    )(*near(*operands))


def merge_kernel(parts, w_out, out):
    count, rows, width = parts.shape
    dim = rows - 16
    tail = [parts[i, dim : dim + 16].astype(F32) for i in range(count)]
    lse = [t[0:1] + t[1:2] + t[2:3] for t in tail]
    top = functools.reduce(jnp.maximum, lse)
    share = [jnp.exp2(v - top) for v in lse]
    whole = functools.reduce(jnp.add, share)
    merged = functools.reduce(
        jnp.add, [parts[i, 0:dim].astype(F32) * share[i] for i in range(count)]
    )
    merged = (merged / whole).astype(BF16)
    heads = w_out.shape[0] // dim
    rows = width // heads
    stacked = jnp.concatenate(
        [merged[:, h * rows : (h + 1) * rows] for h in range(heads)], axis=0
    )
    out[...] = lax.dot_general(
        stacked, w_out[...], (((0,), (0,)), ((), ())), preferred_element_type=F32
    ).astype(BF16)


def body(
    latent,
    condition,
    context_condition,
    context,
    w_shift,
    w_scale,
    w_gate,
    pre_gain,
    post_gain,
    query_gain,
    key_gain,
    w_query,
    w_key,
    w_value,
    w_out,
):
    tp_count = lax.axis_size(TP)
    y_count = lax.axis_size("y")
    model = latent.shape[1]
    head_dim = query_gain.shape[0]
    tok_dev = latent.shape[0] * tp_count
    ctx_dev = context.shape[0]
    heads_dev = w_query.shape[1] // head_dim
    factor = head_dim ** (-0.5) * LOG2E
    lift = math.log(tok_dev / (4.0 * ctx_dev)) * LOG2E

    def receive(value, axis, hop):
        size = lax.axis_size(axis)
        return lax.ppermute(value, axis, [((i + hop) % size, i) for i in range(size)])

    whole = pl.BlockSpec(memory_space=pltpu.VMEM)
    partial_mod = pl.pallas_call(
        modulation_kernel,
        in_specs=[whole] * 5,
        out_specs=whole,
        out_shape=jax.ShapeDtypeStruct((lax.axis_size("z"), 5, w_shift.shape[1]), F32),
        compiler_params=room(16),
        name="modulation",
    )(condition[None], context_condition[None], w_shift, w_scale, w_gate)
    partial_mod = lax.all_to_all(partial_mod, "z", 0, 0, tiled=True)
    partial_mod = partial_mod.sum(axis=0)
    pieces = from_everyone(partial_mod, ("y", *TP))
    mine = [latent] + [receive(latent, "x", h) for h in (1, 2, 3)]
    other = jnp.concatenate(mine, axis=0)
    other = receive(other, "c", 1)

    positions = (lax.axis_index("z") * y_count + lax.axis_index("y")) * tok_dev + jnp.arange(tok_dev)
    cos, sa, sb = rotation_tables(positions, GRID_W, head_dim)
    msg_rows = 2 * tok_dev + 2 * ctx_dev
    place = jnp.stack([lax.axis_index("x"), lax.axis_index("c")]).astype(jnp.int32)
    message, normed, gate = pl.pallas_call(
        project_kernel,
        in_specs=[pl.BlockSpec(memory_space=pltpu.SMEM)] + [whole] * 14,
        out_specs=(whole, whole, whole),
        out_shape=(
            jax.ShapeDtypeStruct((msg_rows, head_dim), BF16),
            pltpu.VMEM((tok_dev, model), BF16),
            jax.ShapeDtypeStruct((1, model), F32),
        ),
        scratch_shapes=[pltpu.VMEM((tok_dev, model), BF16)],
        cost_estimate=pl.CostEstimate(
            flops=2 * tok_dev * model * 2 * head_dim,
            bytes_accessed=2 * model * (2 * head_dim + tok_dev),
            transcendentals=0,
        ),
        compiler_params=room(24),
        name="project",
    )(
        place,
        *near(
            *mine,
            other,
            pieces,
            context,
            pre_gain[None],
            w_key,
            w_value,
            key_gain[None],
            cos,
            sa,
            sb,
        ),
    )
    query = pl.pallas_call(
        query_kernel,
        in_specs=[whole] * 6,
        out_specs=whole,
        out_shape=jax.ShapeDtypeStruct((y_count, head_dim, heads_dev * tok_dev), BF16),
        cost_estimate=pl.CostEstimate(
            flops=2 * tok_dev * model * 2 * head_dim,
            bytes_accessed=2 * model * (2 * head_dim + tok_dev),
            transcendentals=0,
        ),
        compiler_params=room(16),
        name="query",
    )(*near(normed, w_query, query_gain[None], cos, sa, sb))

    far_up, far_down = receive(message, "z", 6), receive(message, "z", -5)
    up, down = receive(message, "z", 1), receive(message, "z", -1)
    q_all = lax.all_to_all(query, "y", 0, 0, tiled=True)
    ups = receive(jnp.concatenate([up, far_up, far_down], axis=0), "z", 1)
    downs = receive(jnp.concatenate([far_up, far_down, down], axis=0), "z", -1)
    last_ups = receive(ups, "z", 1)
    last_downs = receive(downs[: 2 * msg_rows], "z", -1)
    shared = (tok_dev, ctx_dev, factor, lift)
    carry = attend(q_all, [message, up, down, far_up, far_down], None, False, *shared)
    carry = attend(q_all, [ups, downs], carry, False, *shared)
    (partials,) = attend(q_all, [last_ups, last_downs], carry, True, *shared)
    returned = lax.all_to_all(partials, "y", 0, 0, tiled=True)
    mixed = pl.pallas_call(
        merge_kernel,
        out_shape=jax.ShapeDtypeStruct((tok_dev, model), BF16),
        cost_estimate=pl.CostEstimate(
            flops=2 * tok_dev * model * heads_dev * head_dim,
            bytes_accessed=4 * tok_dev * model,
            transcendentals=0,
        ),
        in_specs=[whole, whole],
        out_specs=whole,
        compiler_params=room(16),
        name="merge",
    )(*near(returned, w_out))
    arrived = lax.all_to_all(mixed.reshape(tp_count, -1, model), TP, 0, 0, tiled=True)
    mixed = arrived.astype(F32).sum(axis=0)
    updated = latent.astype(F32) + gate * rms(mixed, post_gain)
    return updated.astype(BF16)


def solution(mesh):
    torus = Mesh(mesh.devices.reshape(16, 4, 4, 2), ALL)
    sp = ("z", "y")
    placed = (
        P(ALL, None),
        P(sp),
        P(sp),
        P(sp, None),
        P(sp, TP),
        P(sp, TP),
        P(sp, TP),
        P(),
        P(),
        P(),
        P(),
        P(None, TP),
        P(None, TP),
        P(None, TP),
        P(TP, None),
    )
    return jax.shard_map(
        body, mesh=torus, in_specs=placed, out_specs=P(ALL, None), check_vma=False
    )
```

```python
import functools
import math

import jax
import jax.numpy as jnp
from jax import lax
from jax.experimental import pallas as pl
from jax.experimental.pallas import tpu as pltpu
from jax.sharding import Mesh
from jax.sharding import PartitionSpec as P

GRID_W = 64
LOG2E = math.log2(math.e)
TP = ("x", "c")
ALL = ("z", "y", *TP)
F32 = jnp.float32
BF16 = jnp.bfloat16


def room(mebibytes):
    return pltpu.CompilerParams(vmem_limit_bytes=mebibytes << 20)


def near(*arrays):
    return [pltpu.with_memory_space_constraint(a, pltpu.VMEM) for a in arrays]


def far(*arrays):
    return [pltpu.with_memory_space_constraint(a, pltpu.HBM) for a in arrays]


def from_everyone(value, axes):
    devices = lax.axis_size(axes)
    return lax.all_to_all(
        jnp.broadcast_to(value[None], (devices, *value.shape)), axes, 0, 0, tiled=True
    )


def rms_rows(values):
    return values * lax.rsqrt(jnp.mean(values * values, axis=-1, keepdims=True) + 1e-06)


def rotation_tables(positions, grid_width, head_dim):
    half = head_dim // 2
    quarter = head_dim // 4
    lane = jnp.arange(head_dim)
    j = (lane % quarter).astype(F32)
    freqs = 10000.0 ** (-(2.0 * j) / half)
    row_pos = (positions // grid_width).astype(F32)[:, None]
    col_pos = (positions % grid_width).astype(F32)[:, None]
    angle = jnp.where(lane[None] < half, row_pos, col_pos) * freqs[None]
    first = ((lane % half) < quarter)[None]
    sine = jnp.sin(angle)
    return (
        jnp.cos(angle),
        jnp.where(first, -sine, 0.0),
        jnp.where(first, 0.0, sine),
    )


def modulation_kernel(cond, ctx_cond, w_shift, w_scale, w_gate, out):
    both = jnp.concatenate([cond[...].astype(F32), ctx_cond[...].astype(F32)], axis=0)
    both = jax.nn.silu(both).astype(BF16)
    shift, scale, gate = (
        jnp.dot(both, w[...], preferred_element_type=F32) for w in (w_shift, w_scale, w_gate)
    )
    rows = jnp.concatenate([shift[0:1], scale[0:1], shift[1:2], scale[1:2], gate[0:1]], axis=0)
    for i in range(out.shape[0]):
        out[i] = rows


def turned(v, gain_row, cos, sa, sb):
    head_dim = v.shape[1]
    quarter = head_dim // 4
    v = rms_rows(v) * gain_row
    up = pltpu.roll(v, head_dim - quarter, 1)
    down = pltpu.roll(v, quarter, 1)
    return v * cos[...] + up * sa[...] + down * sb[...]


def project_kernel(place, *refs):
    mine, other = refs[:4], refs[4]
    pieces, ctx, gain, wk, wv, kg, cos, sa, sb, msg, normed, gate, lat = refs[5:]
    rows = lat.shape[0]
    part = mine[0].shape[0]
    for h in range(4):
        at = jax.lax.rem(place[0] + h, 4) * 2
        lat[pl.ds(pl.multiple_of((at + place[1]) * part, part), part)] = mine[h][...]
        lat[pl.ds(pl.multiple_of((at + 1 - place[1]) * part, part), part)] = other[
            h * part : (h + 1) * part
        ]
    slots = 2 * 4
    mods = jnp.concatenate(
        [
            functools.reduce(
                jnp.add, [pieces[y * slots + t] for y in range(pieces.shape[0] // slots)]
            )
            for t in range(slots)
        ],
        axis=1,
    )
    gate[...] = mods[4:5]
    ctx_rows = ctx.shape[0]
    g = gain[...]
    x = rms_rows(lat[...].astype(F32)) * g
    x = (x * (1.0 + mods[1:2]) + mods[0:1]).astype(BF16)
    normed[...] = x
    c = rms_rows(ctx[...].astype(F32)) * g
    c = (c * (1.0 + mods[3:4]) + mods[2:3]).astype(BF16)
    both = jnp.concatenate([x, c], axis=0)
    k = jnp.dot(both, wk[...], preferred_element_type=F32)
    v = jnp.dot(both, wv[...], preferred_element_type=F32)
    msg[0:rows] = turned(k[:rows], kg[...], cos, sa, sb).astype(BF16)
    msg[rows : 2 * rows] = v[:rows].astype(BF16)
    tail = jnp.concatenate([rms_rows(k[rows:]) * kg[...], v[rows:]], axis=0)
    msg[2 * rows : 2 * rows + 2 * ctx_rows] = tail.astype(BF16)


def query_kernel(normed, wq, qg, cos, sa, sb, q_out):
    rows = normed.shape[0]
    head_dim = qg.shape[1]
    q = jnp.dot(normed[...], wq[...], preferred_element_type=F32)
    for h in range(q.shape[1] // head_dim):
        qh = turned(q[:, h * head_dim : (h + 1) * head_dim], qg[...], cos, sa, sb)
        qt = jnp.transpose(qh).astype(BF16)
        for i in range(q_out.shape[0]):
            q_out[i, :, h * rows : (h + 1) * rows] = qt


def bundle_kernel(*refs, groups):
    outs = refs[-len(groups) :]
    for out, group in zip(outs, groups):
        at = 0
        for k in group:
            rows = min(refs[k].shape[0], out.shape[0] - at)
            out[at : at + rows] = refs[k][0:rows]
            at += rows


def bundled(arrays, groups, rows):
    whole = pl.BlockSpec(memory_space=pltpu.VMEM)
    return pl.pallas_call(
        functools.partial(bundle_kernel, groups=groups),
        in_specs=[whole] * len(arrays),
        out_specs=tuple([whole] * len(groups)),
        out_shape=tuple(
            jax.ShapeDtypeStruct((rows, arrays[0].shape[1]), arrays[0].dtype) for _ in groups
        ),
        compiler_params=room(4),
        name="bundle",
    )(*near(*arrays))


def attend_kernel(*refs, counts, keys, extra, first, last, factor, lift):
    refs = list(refs)
    q = refs.pop(0)
    span = 2 * (keys + extra)
    blocks = []
    for count in counts:
        ref = refs.pop(0)
        blocks += [(ref, i * span) for i in range(count)]
    if not first:
        m_in, l_in, acc_in = refs.pop(0), refs.pop(0), refs.pop(0)
    tails = [ref[at + 2 * keys : at + span].astype(F32) for ref, at in blocks]
    ctx_key = jnp.concatenate([t[:extra] for t in tails], axis=0).astype(BF16)
    ctx_value = jnp.concatenate([t[extra:] for t in tails], axis=0).astype(BF16)

    wide = 2
    width = q.shape[2]

    def both(ref, i):
        return jnp.concatenate([ref[wide * i + w] for w in range(wide)], axis=1)

    def tile(i, unused):
        qv = both(q, i)
        scores = [
            jnp.dot(ref[at : at + keys], qv, preferred_element_type=F32) for ref, at in blocks
        ]
        largest = functools.reduce(
            jnp.maximum, [jnp.max(s, axis=0, keepdims=True) for s in scores]
        )
        ctx_scores = jnp.dot(ctx_key, qv, preferred_element_type=F32) * factor + lift
        largest = jnp.maximum(largest * factor, jnp.max(ctx_scores, axis=0, keepdims=True))
        if not first:
            before = both(m_in, i)
            largest = jnp.maximum(largest, before)
        terms = jnp.exp2(ctx_scores - largest)
        total = jnp.sum(terms, axis=0, keepdims=True)
        acc = weighted(ctx_value, terms)
        if not first:
            fade = jnp.exp2(before - largest)
            total = total + both(l_in, i) * fade
            acc = acc + both(acc_in, i) * fade
        for s, (ref, at) in zip(scores, blocks):
            terms = jnp.exp2(s * factor - largest)
            total = total + jnp.sum(terms, axis=0, keepdims=True)
            acc = acc + weighted(ref[at + keys : at + 2 * keys], terms)
        if last:
            acc = acc / total
            lse = largest + jnp.log2(total)
            hi = lse.astype(BF16).astype(F32)
            mid = (lse - hi).astype(BF16).astype(F32)
            low = lse - hi - mid
            row = lax.broadcasted_iota(jnp.int32, (16, lse.shape[1]), 0)
            packed = jnp.where(
                row == 0, hi, jnp.where(row == 1, mid, jnp.where(row == 2, low, 0.0))
            )
        for w in range(wide):
            at = slice(w * width, (w + 1) * width)
            if last:
                (out,) = refs
                dim = acc.shape[0]
                out[wide * i + w, 0:dim] = acc[:, at].astype(BF16)
                out[wide * i + w, dim : dim + 16] = packed[:, at].astype(BF16)
            else:
                m_out, l_out, acc_out = refs
                m_out[wide * i + w] = largest[:, at]
                l_out[wide * i + w] = total[:, at]
                acc_out[wide * i + w] = acc[:, at]
        return unused

    lax.fori_loop(0, q.shape[0] // wide, tile, 0, unroll=True)


def weighted(values, terms):
    return lax.dot_general(
        values, terms.astype(BF16), (((0,), (0,)), ((), ())), preferred_element_type=F32
    )


def attend(q_all, bundles, carry, last, keys, extra, factor, lift):
    parts, dim, width = q_all.shape
    first = carry is None
    counts = tuple(b.shape[0] // (2 * (keys + extra)) for b in bundles)
    operands = [q_all, *bundles] + ([] if first else list(carry))
    if last:
        out_shape = (jax.ShapeDtypeStruct((parts, dim + 16, width), BF16),)
    else:
        out_shape = (
            pltpu.VMEM((parts, 1, width), F32),
            pltpu.VMEM((parts, 1, width), F32),
            pltpu.VMEM((parts, dim, width), F32),
        )
    whole = pl.BlockSpec(memory_space=pltpu.VMEM)
    all_keys = (keys + extra) * sum(counts)
    return pl.pallas_call(
        functools.partial(
            attend_kernel,
            counts=counts,
            keys=keys,
            extra=extra,
            first=first,
            last=last,
            factor=factor,
            lift=lift,
        ),
        in_specs=[whole] * len(operands),
        out_specs=tuple([whole] * len(out_shape)),
        out_shape=out_shape,
        cost_estimate=pl.CostEstimate(
            flops=4 * all_keys * parts * width * dim,
            bytes_accessed=2 * parts * width * dim * 4,
            transcendentals=all_keys * parts * width,
        ),
        compiler_params=room(32),
        name="attend",
    )(*near(*operands))


def merge_kernel(parts, out):
    count, rows, _ = parts.shape
    dim = rows - 16
    tail = [parts[i, dim : dim + 16].astype(F32) for i in range(count)]
    lse = [t[0:1] + t[1:2] + t[2:3] for t in tail]
    top = functools.reduce(jnp.maximum, lse)
    share = [jnp.exp2(v - top) for v in lse]
    whole = functools.reduce(jnp.add, share)
    merged = functools.reduce(
        jnp.add, [parts[i, 0:dim].astype(F32) * share[i] for i in range(count)]
    )
    merged = merged / whole
    heads = out.shape[2] // dim
    chips, part = out.shape[0], out.shape[1]
    for h in range(heads):
        turn = jnp.transpose(merged[:, h * chips * part : (h + 1) * chips * part]).astype(BF16)
        for i in range(chips):
            out[i, :, h * dim : (h + 1) * dim] = turn[i * part : (i + 1) * part]


def out_kernel(place, attended, w0, w1, w2, w3, mine, other, both, held, done):
    copies = [
        pltpu.make_async_copy(w, held.at[h], done.at[h]) for h, w in enumerate((w0, w1, w2, w3))
    ]
    for copy in copies:
        copy.start()
    for h, copy in enumerate(copies):
        chip = jax.lax.rem(place[0] + h, 4)
        copy.wait()
        partial = jnp.dot(attended[chip], held[h], preferred_element_type=F32)
        partial = partial.astype(BF16).astype(F32)
        both[...] = partial if h == 0 else both[...] + partial
    rows = mine.shape[0]
    mine[...] = both[pl.ds(pl.multiple_of(place[1] * rows, rows), rows)]
    other[...] = both[pl.ds(pl.multiple_of((1 - place[1]) * rows, rows), rows)]


def final_kernel(latent, mine, other, gate, gain, out):
    mixed = mine[...] + other[...]
    out[...] = (latent[...].astype(F32) + gate[...] * (rms_rows(mixed) * gain[...])).astype(BF16)


def body(
    latent,
    condition,
    context_condition,
    context,
    w_shift,
    w_scale,
    w_gate,
    pre_gain,
    post_gain,
    query_gain,
    key_gain,
    w_query,
    w_key,
    w_value,
    w_out,
):
    tp_count = lax.axis_size(TP)
    y_count = lax.axis_size("y")
    model = latent.shape[1]
    head_dim = query_gain.shape[0]
    tok_dev = latent.shape[0] * tp_count
    ctx_dev = context.shape[0]
    heads_dev = w_query.shape[1] // head_dim
    factor = head_dim ** (-0.5) * LOG2E
    lift = math.log(tok_dev / (4.0 * ctx_dev)) * LOG2E

    def receive(value, axis, hop):
        size = lax.axis_size(axis)
        return lax.ppermute(value, axis, [((i + hop) % size, i) for i in range(size)])

    whole = pl.BlockSpec(memory_space=pltpu.VMEM)
    partial_mod = pl.pallas_call(
        modulation_kernel,
        in_specs=[whole] * 5,
        out_specs=whole,
        out_shape=jax.ShapeDtypeStruct((lax.axis_size("z"), 5, w_shift.shape[1]), F32),
        compiler_params=room(16),
        name="modulation",
    )(*far(condition[None], context_condition[None], w_shift, w_scale, w_gate))
    partial_mod = lax.all_to_all(partial_mod, "z", 0, 0, tiled=True)
    partial_mod = partial_mod.sum(axis=0)
    pieces = from_everyone(partial_mod, ("y", *TP))
    mine = [latent] + [receive(latent, "x", h) for h in (1, 2, 3)]
    other = jnp.concatenate(mine, axis=0)
    other = receive(other, "c", 1)

    positions = (lax.axis_index("z") * y_count + lax.axis_index("y")) * tok_dev + jnp.arange(tok_dev)
    cos, sa, sb = rotation_tables(positions, GRID_W, head_dim)
    msg_rows = 2 * tok_dev + 2 * ctx_dev
    place = jnp.stack([lax.axis_index("x"), lax.axis_index("c")]).astype(jnp.int32)
    message, normed, gate = pl.pallas_call(
        project_kernel,
        in_specs=[pl.BlockSpec(memory_space=pltpu.SMEM)] + [whole] * 14,
        out_specs=(whole, whole, whole),
        out_shape=(
            jax.ShapeDtypeStruct((msg_rows, head_dim), BF16),
            pltpu.VMEM((tok_dev, model), BF16),
            jax.ShapeDtypeStruct((1, model), F32),
        ),
        scratch_shapes=[pltpu.VMEM((tok_dev, model), BF16)],
        cost_estimate=pl.CostEstimate(
            flops=2 * tok_dev * model * 2 * head_dim,
            bytes_accessed=2 * model * (2 * head_dim + tok_dev),
            transcendentals=0,
        ),
        compiler_params=room(24),
        name="project",
    )(
        place,
        *near(
            *mine,
            other,
            pieces,
            context,
            pre_gain[None],
            w_key,
            w_value,
            key_gain[None],
            cos,
            sa,
            sb,
        ),
    )
    query = pl.pallas_call(
        query_kernel,
        in_specs=[whole] * 6,
        out_specs=whole,
        out_shape=jax.ShapeDtypeStruct((y_count, head_dim, heads_dev * tok_dev), BF16),
        cost_estimate=pl.CostEstimate(
            flops=2 * tok_dev * model * 2 * head_dim,
            bytes_accessed=2 * model * (2 * head_dim + tok_dev),
            transcendentals=0,
        ),
        compiler_params=room(16),
        name="query",
    )(*near(normed, w_query, query_gain[None], cos, sa, sb))

    far_up, far_down = receive(message, "z", 6), receive(message, "z", -5)
    up, down = receive(message, "z", 1), receive(message, "z", -1)
    q_all = lax.all_to_all(query, "y", 0, 0, tiled=True)
    w_outs = [w_out] + [receive(w_out, "x", h) for h in (1, 2, 3)]
    to_down, to_up = bundled(
        [up, far_up, far_down, down], ((0, 1, 2), (1, 2, 3)), 3 * msg_rows
    )
    ups, downs = receive(to_down, "z", 1), receive(to_up, "z", -1)
    last_ups = receive(ups, "z", 1)
    (to_up,) = bundled([downs], ((0,),), 2 * msg_rows)
    last_downs = receive(to_up, "z", -1)
    shared = (tok_dev, ctx_dev, factor, lift)
    carry = attend(q_all, [message, up, down, far_up, far_down], None, False, *shared)
    carry = attend(q_all, [ups, downs], carry, False, *shared)
    (partials,) = attend(q_all, [last_ups, last_downs], carry, True, *shared)
    returned = lax.all_to_all(partials, "y", 0, 0, tiled=True)
    attended = pl.pallas_call(
        merge_kernel,
        in_specs=[whole],
        out_specs=whole,
        out_shape=jax.ShapeDtypeStruct(
            (lax.axis_size("x"), tok_dev // lax.axis_size("x"), heads_dev * head_dim), BF16
        ),
        compiler_params=room(16),
        name="merge",
    )(*near(returned))
    attended = lax.all_to_all(attended, "x", 0, 0, tiled=True)
    rows = latent.shape[0]
    sums, others = pl.pallas_call(
        out_kernel,
        in_specs=[pl.BlockSpec(memory_space=pltpu.SMEM), whole]
        + [pl.BlockSpec(memory_space=pltpu.HBM)] * 4,
        out_specs=(whole, whole),
        out_shape=(
            jax.ShapeDtypeStruct((rows, model), F32),
            jax.ShapeDtypeStruct((rows, model), F32),
        ),
        scratch_shapes=[
            pltpu.VMEM((2 * rows, model), F32),
            pltpu.VMEM((4, *w_out.shape), BF16),
            pltpu.SemaphoreType.DMA((4,)),
        ],
        compiler_params=room(16),
        cost_estimate=pl.CostEstimate(
            flops=2 * tok_dev * model * heads_dev * head_dim,
            bytes_accessed=4 * tok_dev * model,
            transcendentals=0,
        ),
        name="out",
    )(place, *near(attended), *far(*w_outs))
    others = receive(others, "c", 1)
    return pl.pallas_call(
        final_kernel,
        in_specs=[whole] * 5,
        out_specs=whole,
        out_shape=jax.ShapeDtypeStruct((rows, model), BF16),
        compiler_params=room(16),
        name="final",
    )(*near(latent, sums, others, gate, post_gain[None]))


def solution(mesh):
    torus = Mesh(mesh.devices.reshape(16, 4, 4, 2), ALL)
    sp = ("z", "y")
    placed = (
        P(ALL, None),
        P(sp),
        P(sp),
        P(sp, None),
        P(sp, TP),
        P(sp, TP),
        P(sp, TP),
        P(),
        P(),
        P(),
        P(),
        P(None, TP),
        P(None, TP),
        P(None, TP),
        P(TP, None),
    )
    return jax.shard_map(body, mesh=torus, in_specs=placed, out_specs=P(ALL, None), check_vma=False)
```

```python
import functools
import math

import jax
import jax.numpy as jnp
from jax import lax
from jax.experimental import pallas as pl
from jax.experimental.pallas import tpu as pltpu
from jax.sharding import Mesh
from jax.sharding import PartitionSpec as P

GRID_W = 64
LOG2E = math.log2(math.e)
TP = ("x", "c")
ALL = ("z", "y", *TP)
F32 = jnp.float32
BF16 = jnp.bfloat16


def room(mebibytes):
    return pltpu.CompilerParams(vmem_limit_bytes=mebibytes << 20)


def near(*arrays):
    return [pltpu.with_memory_space_constraint(a, pltpu.VMEM) for a in arrays]


def far(*arrays):
    return [pltpu.with_memory_space_constraint(a, pltpu.HBM) for a in arrays]


def rms_rows(values):
    return values * lax.rsqrt(jnp.mean(values * values, axis=-1, keepdims=True) + 1e-06)


def rotation_tables(positions, grid_width, head_dim):
    half = head_dim // 2
    quarter = head_dim // 4
    lane = jnp.arange(head_dim)
    j = (lane % quarter).astype(F32)
    freqs = 10000.0 ** (-(2.0 * j) / half)
    row_pos = (positions // grid_width).astype(F32)[:, None]
    col_pos = (positions % grid_width).astype(F32)[:, None]
    angle = jnp.where(lane[None] < half, row_pos, col_pos) * freqs[None]
    first = ((lane % half) < quarter)[None]
    sine = jnp.sin(angle)
    return (
        jnp.cos(angle),
        jnp.where(first, -sine, 0.0),
        jnp.where(first, 0.0, sine),
    )


def modulation_kernel(cond, ctx_cond, w_shift, w_scale, w_gate, out):
    both = jnp.concatenate([cond[...].astype(F32), ctx_cond[...].astype(F32)], axis=0)
    both = jax.nn.silu(both).astype(BF16)
    shift, scale, gate = (
        jnp.dot(both, w[...], preferred_element_type=F32) for w in (w_shift, w_scale, w_gate)
    )
    rows = jnp.concatenate([shift[0:1], scale[0:1], shift[1:2], scale[1:2], gate[0:1]], axis=0)
    for i in range(out.shape[0]):
        out[i] = rows


def turned(v, gain_row, cos, sa, sb):
    head_dim = v.shape[1]
    quarter = head_dim // 4
    v = rms_rows(v) * gain_row
    up = pltpu.roll(v, head_dim - quarter, 1)
    down = pltpu.roll(v, quarter, 1)
    return v * cos[...] + up * sa[...] + down * sb[...]


def project_kernel(place, *refs):
    mine, other = refs[:4], refs[4]
    pieces, ctx, gain, wk, wv, gains, cos, sa, sb, msg, normed, gate, lat = refs[5:]
    rows = lat.shape[0]
    part = mine[0].shape[0]
    for h in range(4):
        at = jax.lax.rem(place[0] + h, 4) * 2
        lat[pl.ds(pl.multiple_of((at + place[1]) * part, part), part)] = mine[h][...]
        lat[pl.ds(pl.multiple_of((at + 1 - place[1]) * part, part), part)] = other[
            h * part : (h + 1) * part
        ]
    slots = 2 * 4
    mods = jnp.concatenate(
        [
            functools.reduce(
                jnp.add, [pieces[y * slots + t] for y in range(pieces.shape[0] // slots)]
            )
            for t in range(slots)
        ],
        axis=1,
    )
    gate[...] = mods[4:5]
    ctx_rows = ctx.shape[0]
    g = gain[...]
    x = rms_rows(lat[...].astype(F32)) * g
    x = (x * (1.0 + mods[1:2]) + mods[0:1]).astype(BF16)
    normed[...] = x
    c = rms_rows(ctx[...].astype(F32)) * g
    c = (c * (1.0 + mods[3:4]) + mods[2:3]).astype(BF16)
    both = jnp.concatenate([x, c], axis=0)
    k = jnp.dot(both, wk[...], preferred_element_type=F32)
    v = jnp.dot(both, wv[...], preferred_element_type=F32)
    msg[0:rows] = turned(k[:rows], gains[1:2], cos, sa, sb).astype(BF16)
    msg[rows : 2 * rows] = v[:rows].astype(BF16)
    tail = jnp.concatenate([rms_rows(k[rows:]) * gains[1:2], v[rows:]], axis=0)
    msg[2 * rows : 2 * rows + 2 * ctx_rows] = tail.astype(BF16)


def query_kernel(normed, wq, gains, cos, sa, sb, q_out, *, chips):
    head_dim = gains.shape[1]
    q = jnp.dot(normed[...], wq[...], preferred_element_type=F32)
    heads = [
        turned(q[:, h : h + head_dim], gains[0:1], cos, sa, sb)
        for h in range(0, q.shape[1], head_dim)
    ]
    part = q.shape[0] // chips
    rows = [v[i * part : (i + 1) * part] for i in range(chips) for v in heads]
    qt = jnp.transpose(jnp.concatenate(rows, axis=0)).astype(BF16)
    for i in range(q_out.shape[0]):
        q_out[i] = qt


def spread_kernel(blocks, out):
    total = functools.reduce(jnp.add, [blocks[i] for i in range(blocks.shape[0])])
    for i in range(out.shape[0]):
        out[i] = total


def bundle_kernel(*refs, groups):
    outs = refs[-len(groups) :]
    for out, group in zip(outs, groups):
        at = 0
        for k in group:
            rows = min(refs[k].shape[0], out.shape[0] - at)
            out[at : at + rows] = refs[k][0:rows]
            at += rows


def bundled(arrays, groups, rows):
    whole = pl.BlockSpec(memory_space=pltpu.VMEM)
    return pl.pallas_call(
        functools.partial(bundle_kernel, groups=groups),
        in_specs=[whole] * len(arrays),
        out_specs=tuple([whole] * len(groups)),
        out_shape=tuple(
            jax.ShapeDtypeStruct((rows, arrays[0].shape[1]), arrays[0].dtype) for _ in groups
        ),
        compiler_params=room(4),
        name="bundle",
    )(*near(*arrays))


def attend_kernel(*refs, counts, keys, extra, first, last, factor, lift):
    refs = list(refs)
    q = refs.pop(0)
    span = 2 * (keys + extra)
    blocks = []
    for count in counts:
        ref = refs.pop(0)
        blocks += [(ref, i * span) for i in range(count)]
    if not first:
        m_in, l_in, acc_in = refs.pop(0), refs.pop(0), refs.pop(0)
    tails = [ref[at + 2 * keys : at + span].astype(F32) for ref, at in blocks]
    ctx_key = jnp.concatenate([t[:extra] for t in tails], axis=0).astype(BF16)
    ctx_value = jnp.concatenate([t[extra:] for t in tails], axis=0).astype(BF16)

    wide = 2
    width = q.shape[2]

    def both(ref, i):
        return jnp.concatenate([ref[wide * i + w] for w in range(wide)], axis=1)

    def tile(i, unused):
        qv = both(q, i)
        scores = [
            jnp.dot(ref[at : at + keys], qv, preferred_element_type=F32) for ref, at in blocks
        ]
        largest = functools.reduce(
            jnp.maximum, [jnp.max(s, axis=0, keepdims=True) for s in scores]
        )
        ctx_scores = jnp.dot(ctx_key, qv, preferred_element_type=F32) * factor + lift
        largest = jnp.maximum(largest * factor, jnp.max(ctx_scores, axis=0, keepdims=True))
        if not first:
            before = both(m_in, i)
            largest = jnp.maximum(largest, before)
        terms = jnp.exp2(ctx_scores - largest)
        total = jnp.sum(terms, axis=0, keepdims=True)
        acc = weighted(ctx_value, terms)
        if not first:
            fade = jnp.exp2(before - largest)
            total = total + both(l_in, i) * fade
            acc = acc + both(acc_in, i) * fade
        for s, (ref, at) in zip(scores, blocks):
            terms = jnp.exp2(s * factor - largest)
            total = total + jnp.sum(terms, axis=0, keepdims=True)
            acc = acc + weighted(ref[at + keys : at + 2 * keys], terms)
        if last:
            acc = acc / total
            lse = largest + jnp.log2(total)
            hi = lse.astype(BF16).astype(F32)
            mid = (lse - hi).astype(BF16).astype(F32)
            low = lse - hi - mid
            row = lax.broadcasted_iota(jnp.int32, (16, lse.shape[1]), 0)
            packed = jnp.where(
                row == 0, hi, jnp.where(row == 1, mid, jnp.where(row == 2, low, 0.0))
            )
        for w in range(wide):
            at = slice(w * width, (w + 1) * width)
            if last:
                (out,) = refs
                dim, lanes = acc.shape[0], out.shape[2]
                for n in range(width // lanes):
                    at = slice(w * width + n * lanes, w * width + (n + 1) * lanes)
                    to = (wide * i + w) * (width // lanes) + n
                    out[to, 0:dim] = acc[:, at].astype(BF16)
                    out[to, dim : dim + 16] = packed[:, at].astype(BF16)
            else:
                m_out, l_out, acc_out = refs
                m_out[wide * i + w] = largest[:, at]
                l_out[wide * i + w] = total[:, at]
                acc_out[wide * i + w] = acc[:, at]
        return unused

    lax.fori_loop(0, q.shape[0] // wide, tile, 0, unroll=True)


def weighted(values, terms):
    return lax.dot_general(
        values, terms.astype(BF16), (((0,), (0,)), ((), ())), preferred_element_type=F32
    )


def attend(q_all, bundles, carry, last, keys, extra, factor, lift, chips):
    parts, dim, width = q_all.shape
    first = carry is None
    counts = tuple(b.shape[0] // (2 * (keys + extra)) for b in bundles)
    operands = [q_all, *bundles] + ([] if first else list(carry))
    if last:
        out_shape = (jax.ShapeDtypeStruct((parts * chips, dim + 16, width // chips), BF16),)
    else:
        out_shape = (
            pltpu.VMEM((parts, 1, width), F32),
            pltpu.VMEM((parts, 1, width), F32),
            pltpu.VMEM((parts, dim, width), F32),
        )
    whole = pl.BlockSpec(memory_space=pltpu.VMEM)
    all_keys = (keys + extra) * sum(counts)
    return pl.pallas_call(
        functools.partial(
            attend_kernel,
            counts=counts,
            keys=keys,
            extra=extra,
            first=first,
            last=last,
            factor=factor,
            lift=lift,
        ),
        in_specs=[whole] * len(operands),
        out_specs=tuple([whole] * len(out_shape)),
        out_shape=out_shape,
        cost_estimate=pl.CostEstimate(
            flops=4 * all_keys * parts * width * dim,
            bytes_accessed=2 * parts * width * dim * 4,
            transcendentals=all_keys * parts * width,
        ),
        compiler_params=room(32),
        name="attend",
    )(*near(*operands))


def out_kernel(place, parts, w0, w1, w2, w3, mine, other, both, held, done):
    copies = [
        pltpu.make_async_copy(w, held.at[h], done.at[h]) for h, w in enumerate((w0, w1, w2, w3))
    ]
    for copy in copies:
        copy.start()
    chips = len(copies)
    dim = parts.shape[1] - 16
    rows = mine.shape[0]
    for h, copy in enumerate(copies):
        chip = jax.lax.rem(place[0] + h, chips)
        group = [y * chips + chip for y in range(parts.shape[0] // chips)]
        tail = [parts[i, dim : dim + 16].astype(F32) for i in group]
        lse = [t[0:1] + t[1:2] + t[2:3] for t in tail]
        top = functools.reduce(jnp.maximum, lse)
        share = [jnp.exp2(v - top) for v in lse]
        whole = functools.reduce(jnp.add, share)
        merged = functools.reduce(
            jnp.add, [parts[i, 0:dim].astype(F32) * s for i, s in zip(group, share)]
        )
        turn = jnp.transpose(merged / whole)
        attended = jnp.concatenate(
            [turn[at : at + 2 * rows] for at in range(0, turn.shape[0], 2 * rows)], axis=1
        ).astype(BF16)
        copy.wait()
        partial = jnp.dot(attended, held[h], preferred_element_type=F32)
        partial = partial.astype(BF16).astype(F32)
        both[...] = partial if h == 0 else both[...] + partial
    mine[...] = both[pl.ds(pl.multiple_of(place[1] * rows, rows), rows)]
    other[...] = both[pl.ds(pl.multiple_of((1 - place[1]) * rows, rows), rows)]


def final_kernel(latent, mine, other, gate, gain, out):
    mixed = mine[...] + other[...]
    out[...] = (latent[...].astype(F32) + gate[...] * (rms_rows(mixed) * gain[...])).astype(BF16)


def body(
    latent,
    condition,
    context_condition,
    context,
    w_shift,
    w_scale,
    w_gate,
    pre_gain,
    post_gain,
    query_gain,
    key_gain,
    w_query,
    w_key,
    w_value,
    w_out,
):
    tp_count = lax.axis_size(TP)
    y_count = lax.axis_size("y")
    model = latent.shape[1]
    head_dim = query_gain.shape[0]
    tok_dev = latent.shape[0] * tp_count
    ctx_dev = context.shape[0]
    heads_dev = w_query.shape[1] // head_dim
    factor = head_dim ** (-0.5) * LOG2E
    lift = math.log(tok_dev / (4.0 * ctx_dev)) * LOG2E

    def receive(value, axis, hop):
        size = lax.axis_size(axis)
        return lax.ppermute(value, axis, [((i + hop) % size, i) for i in range(size)])

    chips = lax.axis_size("x")
    whole = pl.BlockSpec(memory_space=pltpu.VMEM)
    gains = jnp.stack([query_gain, key_gain])
    partial_mod = pl.pallas_call(
        modulation_kernel,
        in_specs=[whole] * 5,
        out_specs=whole,
        out_shape=jax.ShapeDtypeStruct((lax.axis_size("z"), 5, w_shift.shape[1]), F32),
        compiler_params=room(16),
        name="modulation",
    )(*far(condition[None], context_condition[None], w_shift, w_scale, w_gate))
    partial_mod = lax.all_to_all(partial_mod, "z", 0, 0, tiled=True)
    partial_mod = pl.pallas_call(
        spread_kernel,
        in_specs=[whole],
        out_specs=whole,
        out_shape=jax.ShapeDtypeStruct((y_count * tp_count, *partial_mod.shape[1:]), F32),
        compiler_params=room(4),
        name="spread",
    )(*near(partial_mod))
    pieces = lax.all_to_all(partial_mod, ("y", *TP), 0, 0, tiled=True)
    mine = [latent] + [receive(latent, "x", h) for h in (1, 2, 3)]
    other = jnp.concatenate(mine, axis=0)
    other = receive(other, "c", 1)

    positions = (lax.axis_index("z") * y_count + lax.axis_index("y")) * tok_dev + jnp.arange(tok_dev)
    cos, sa, sb = rotation_tables(positions, GRID_W, head_dim)
    msg_rows = 2 * tok_dev + 2 * ctx_dev
    place = jnp.stack([lax.axis_index("x"), lax.axis_index("c")]).astype(jnp.int32)
    message, normed, gate = pl.pallas_call(
        project_kernel,
        in_specs=[pl.BlockSpec(memory_space=pltpu.SMEM)] + [whole] * 14,
        out_specs=(whole, whole, whole),
        out_shape=(
            jax.ShapeDtypeStruct((msg_rows, head_dim), BF16),
            pltpu.VMEM((tok_dev, model), BF16),
            jax.ShapeDtypeStruct((1, model), F32),
        ),
        scratch_shapes=[pltpu.VMEM((tok_dev, model), BF16)],
        cost_estimate=pl.CostEstimate(
            flops=2 * tok_dev * model * 2 * head_dim,
            bytes_accessed=2 * model * (2 * head_dim + tok_dev),
            transcendentals=0,
        ),
        compiler_params=room(24),
        name="project",
    )(
        place,
        *near(
            *mine,
            other,
            pieces,
            context,
            pre_gain[None],
            w_key,
            w_value,
            gains,
            cos,
            sa,
            sb,
        ),
    )
    query = pl.pallas_call(
        functools.partial(query_kernel, chips=chips),
        in_specs=[whole] * 6,
        out_specs=whole,
        out_shape=jax.ShapeDtypeStruct((y_count, head_dim, heads_dev * tok_dev), BF16),
        cost_estimate=pl.CostEstimate(
            flops=2 * tok_dev * model * 2 * head_dim,
            bytes_accessed=2 * model * (2 * head_dim + tok_dev),
            transcendentals=0,
        ),
        compiler_params=room(16),
        name="query",
    )(*near(normed, w_query, gains, cos, sa, sb))

    far_up, far_down = receive(message, "z", 6), receive(message, "z", -5)
    up, down = receive(message, "z", 1), receive(message, "z", -1)
    q_all = lax.all_to_all(query, "y", 0, 0, tiled=True)
    w_outs = [w_out] + [receive(w_out, "x", h) for h in (1, 2, 3)]
    to_down, to_up = bundled(
        [up, far_up, far_down, down], ((0, 1, 2), (1, 2, 3)), 3 * msg_rows
    )
    ups, downs = receive(to_down, "z", 1), receive(to_up, "z", -1)
    last_ups = receive(ups, "z", 1)
    (to_up,) = bundled([downs], ((0,),), 2 * msg_rows)
    last_downs = receive(to_up, "z", -1)
    shared = (tok_dev, ctx_dev, factor, lift, chips)
    carry = attend(q_all, [message, up, down, far_up, far_down], None, False, *shared)
    carry = attend(q_all, [ups, downs], carry, False, *shared)
    (partials,) = attend(q_all, [last_ups, last_downs], carry, True, *shared)
    returned = lax.all_to_all(partials, ("y", "x"), 0, 0, tiled=True)
    rows = latent.shape[0]
    sums, others = pl.pallas_call(
        out_kernel,
        in_specs=[pl.BlockSpec(memory_space=pltpu.SMEM), whole]
        + [pl.BlockSpec(memory_space=pltpu.HBM)] * 4,
        out_specs=(whole, whole),
        out_shape=(
            jax.ShapeDtypeStruct((rows, model), F32),
            jax.ShapeDtypeStruct((rows, model), F32),
        ),
        scratch_shapes=[
            pltpu.VMEM((2 * rows, model), F32),
            pltpu.VMEM((4, *w_out.shape), BF16),
            pltpu.SemaphoreType.DMA((4,)),
        ],
        compiler_params=room(16),
        cost_estimate=pl.CostEstimate(
            flops=2 * tok_dev * model * heads_dev * head_dim,
            bytes_accessed=4 * tok_dev * model,
            transcendentals=0,
        ),
        name="out",
    )(place, *near(returned), *far(*w_outs))
    others = receive(others, "c", 1)
    return pl.pallas_call(
        final_kernel,
        in_specs=[whole] * 5,
        out_specs=whole,
        out_shape=jax.ShapeDtypeStruct((rows, model), BF16),
        compiler_params=room(16),
        name="final",
    )(*near(latent, sums, others, gate, post_gain[None]))


def solution(mesh):
    torus = Mesh(mesh.devices.reshape(16, 4, 4, 2), ALL)
    sp = ("z", "y")
    placed = (
        P(ALL, None),
        P(sp),
        P(sp),
        P(sp, None),
        P(sp, TP),
        P(sp, TP),
        P(sp, TP),
        P(),
        P(),
        P(),
        P(),
        P(None, TP),
        P(None, TP),
        P(None, TP),
        P(TP, None),
    )
    return jax.shard_map(body, mesh=torus, in_specs=placed, out_specs=P(ALL, None), check_vma=False)
```

```python
import functools
import math

import jax
import jax.numpy as jnp
from jax import lax
from jax.experimental import pallas as pl
from jax.experimental.pallas import tpu as pltpu
from jax.sharding import Mesh
from jax.sharding import PartitionSpec as P


GRID_W = 64
LOG2E = math.log2(math.e)
TP = ("x", "c")
ALL = ("z", "y", *TP)
F32 = jnp.float32
BF16 = jnp.bfloat16


def room(mebibytes):
    return pltpu.CompilerParams(vmem_limit_bytes=mebibytes << 20)


def near(*arrays):
    return [pltpu.with_memory_space_constraint(a, pltpu.VMEM) for a in arrays]


def far(*arrays):
    return [pltpu.with_memory_space_constraint(a, pltpu.HBM) for a in arrays]


def rms_rows(values):
    return values * lax.rsqrt(jnp.mean(values * values, axis=-1, keepdims=True) + 1e-06)


def rotation_tables(positions, grid_width, head_dim):
    half = head_dim // 2
    quarter = head_dim // 4
    lane = jnp.arange(head_dim)
    j = (lane % quarter).astype(F32)
    freqs = 10000.0 ** (-(2.0 * j) / half)
    row_pos = (positions // grid_width).astype(F32)[:, None]
    col_pos = (positions % grid_width).astype(F32)[:, None]
    angle = jnp.where(lane[None] < half, row_pos, col_pos) * freqs[None]
    first = ((lane % half) < quarter)[None]
    sine = jnp.sin(angle)
    return (
        jnp.cos(angle),
        jnp.where(first, -sine, 0.0),
        jnp.where(first, 0.0, sine),
    )


def modulation_kernel(cond, ctx_cond, w_shift, w_scale, w_gate, out):
    both = jnp.concatenate([cond[...].astype(F32), ctx_cond[...].astype(F32)], axis=0)
    both = jax.nn.silu(both).astype(BF16)
    shift, scale, gate = (
        jnp.dot(both, w[...], preferred_element_type=F32) for w in (w_shift, w_scale, w_gate)
    )
    rows = jnp.concatenate([shift[0:1], scale[0:1], shift[1:2], scale[1:2], gate[0:1]], axis=0)
    for i in range(out.shape[0]):
        out[i] = rows


def turned(v, gain_row, cos, sa, sb):
    head_dim = v.shape[1]
    quarter = head_dim // 4
    v = rms_rows(v) * gain_row
    up = pltpu.roll(v, head_dim - quarter, 1)
    down = pltpu.roll(v, quarter, 1)
    return v * cos[...] + up * sa[...] + down * sb[...]


def project_kernel(place, *refs):
    mine, other = refs[:4], refs[4]
    pieces, ctx, gain, wk, wv, gains, cos, sa, sb, msg, normed, gate, lat = refs[5:]
    rows = lat.shape[0]
    part = mine[0].shape[0]
    for h in range(4):
        at = jax.lax.rem(place[0] + h, 4) * 2
        lat[pl.ds(pl.multiple_of((at + place[1]) * part, part), part)] = mine[h][...]
        lat[pl.ds(pl.multiple_of((at + 1 - place[1]) * part, part), part)] = other[
            h * part : (h + 1) * part
        ]
    slots = 2 * 4
    mods = jnp.concatenate(
        [
            functools.reduce(
                jnp.add, [pieces[y * slots + t] for y in range(pieces.shape[0] // slots)]
            )
            for t in range(slots)
        ],
        axis=1,
    )
    gate[...] = mods[4:5]
    ctx_rows = ctx.shape[0]
    g = gain[...]
    x = rms_rows(lat[...].astype(F32)) * g
    x = (x * (1.0 + mods[1:2]) + mods[0:1]).astype(BF16)
    normed[...] = x
    c = rms_rows(ctx[...].astype(F32)) * g
    c = (c * (1.0 + mods[3:4]) + mods[2:3]).astype(BF16)
    both = jnp.concatenate([x, c], axis=0)
    k = jnp.dot(both, wk[...], preferred_element_type=F32)
    v = jnp.dot(both, wv[...], preferred_element_type=F32)
    msg[0:rows] = turned(k[:rows], gains[1:2], cos, sa, sb).astype(BF16)
    msg[rows : 2 * rows] = v[:rows].astype(BF16)
    tail = jnp.concatenate([rms_rows(k[rows:]) * gains[1:2], v[rows:]], axis=0)
    msg[2 * rows : 2 * rows + 2 * ctx_rows] = tail.astype(BF16)


def query_kernel(normed, wq, gains, cos, sa, sb, q_out, *, chips):
    head_dim = gains.shape[1]
    q = jnp.dot(normed[...], wq[...], preferred_element_type=F32)
    heads = [
        turned(q[:, h : h + head_dim], gains[0:1], cos, sa, sb)
        for h in range(0, q.shape[1], head_dim)
    ]
    part = q.shape[0] // chips
    rows = [v[i * part : (i + 1) * part] for i in range(chips) for v in heads]
    qt = jnp.transpose(jnp.concatenate(rows, axis=0)).astype(BF16)
    for i in range(q_out.shape[0]):
        q_out[i] = qt


def spread_kernel(blocks, out):
    total = functools.reduce(jnp.add, [blocks[i] for i in range(blocks.shape[0])])
    for i in range(out.shape[0]):
        out[i] = total


def bundle_kernel(*refs, groups):
    outs = refs[-len(groups) :]
    for out, group in zip(outs, groups):
        at = 0
        for k in group:
            rows = min(refs[k].shape[0], out.shape[0] - at)
            out[at : at + rows] = refs[k][0:rows]
            at += rows


def bundled(arrays, groups, rows):
    whole = pl.BlockSpec(memory_space=pltpu.VMEM)
    return pl.pallas_call(
        functools.partial(bundle_kernel, groups=groups),
        in_specs=[whole] * len(arrays),
        out_specs=tuple([whole] * len(groups)),
        out_shape=tuple(
            jax.ShapeDtypeStruct((rows, arrays[0].shape[1]), arrays[0].dtype) for _ in groups
        ),
        compiler_params=room(4),
        name="bundle",
    )(*near(*arrays))


def attend_kernel(*refs, counts, keys, extra, first, last, factor, lift):
    refs = list(refs)
    q = refs.pop(0)
    span = 2 * (keys + extra)
    blocks = []
    for count in counts:
        ref = refs.pop(0)
        blocks += [(ref, i * span) for i in range(count)]
    if not first:
        m_in, l_in, acc_in = refs.pop(0), refs.pop(0), refs.pop(0)
    tails = [ref[at + 2 * keys : at + span].astype(F32) for ref, at in blocks]
    ctx_key = jnp.concatenate([t[:extra] for t in tails], axis=0).astype(BF16)
    ctx_value = jnp.concatenate([t[extra:] for t in tails], axis=0).astype(BF16)

    wide = 2
    width = q.shape[2]

    def both(ref, i):
        return jnp.concatenate([ref[wide * i + w] for w in range(wide)], axis=1)

    def tile(i, unused):
        qv = both(q, i)
        scores = [
            jnp.dot(ref[at : at + keys], qv, preferred_element_type=F32) for ref, at in blocks
        ]
        largest = functools.reduce(
            jnp.maximum, [jnp.max(s, axis=0, keepdims=True) for s in scores]
        )
        ctx_scores = jnp.dot(ctx_key, qv, preferred_element_type=F32) * factor + lift
        largest = jnp.maximum(largest * factor, jnp.max(ctx_scores, axis=0, keepdims=True))
        if not first:
            before = both(m_in, i)
            largest = jnp.maximum(largest, before)
        terms = jnp.exp2(ctx_scores - largest)
        total = jnp.sum(terms, axis=0, keepdims=True)
        acc = weighted(ctx_value, terms)
        if not first:
            fade = jnp.exp2(before - largest)
            total = total + both(l_in, i) * fade
            acc = acc + both(acc_in, i) * fade
        for s, (ref, at) in zip(scores, blocks):
            terms = jnp.exp2(s * factor - largest)
            total = total + jnp.sum(terms, axis=0, keepdims=True)
            acc = acc + weighted(ref[at + keys : at + 2 * keys], terms)
        if last:
            acc = acc / total
            lse = largest + jnp.log2(total)
            hi = lse.astype(BF16).astype(F32)
            mid = (lse - hi).astype(BF16).astype(F32)
            low = lse - hi - mid
            row = lax.broadcasted_iota(jnp.int32, (16, lse.shape[1]), 0)
            packed = jnp.where(
                row == 0, hi, jnp.where(row == 1, mid, jnp.where(row == 2, low, 0.0))
            )
        for w in range(wide):
            at = slice(w * width, (w + 1) * width)
            if last:
                (out,) = refs
                dim, lanes = acc.shape[0], out.shape[2]
                for n in range(width // lanes):
                    at = slice(w * width + n * lanes, w * width + (n + 1) * lanes)
                    to = (wide * i + w) * (width // lanes) + n
                    out[to, 0:dim] = acc[:, at].astype(BF16)
                    out[to, dim : dim + 16] = packed[:, at].astype(BF16)
            else:
                m_out, l_out, acc_out = refs
                m_out[wide * i + w] = largest[:, at]
                l_out[wide * i + w] = total[:, at]
                acc_out[wide * i + w] = acc[:, at]
        return unused

    lax.fori_loop(0, q.shape[0] // wide, tile, 0, unroll=True)


def weighted(values, terms):
    return lax.dot_general(
        values, terms.astype(BF16), (((0,), (0,)), ((), ())), preferred_element_type=F32
    )


def attend(q_all, bundles, carry, last, keys, extra, factor, lift, chips):
    parts, dim, width = q_all.shape
    first = carry is None
    counts = tuple(b.shape[0] // (2 * (keys + extra)) for b in bundles)
    operands = [q_all, *bundles] + ([] if first else list(carry))
    if last:
        out_shape = (jax.ShapeDtypeStruct((parts * chips, dim + 16, width // chips), BF16),)
    else:
        out_shape = (
            pltpu.VMEM((parts, 1, width), F32),
            pltpu.VMEM((parts, 1, width), F32),
            pltpu.VMEM((parts, dim, width), F32),
        )
    whole = pl.BlockSpec(memory_space=pltpu.VMEM)
    all_keys = (keys + extra) * sum(counts)
    return pl.pallas_call(
        functools.partial(
            attend_kernel,
            counts=counts,
            keys=keys,
            extra=extra,
            first=first,
            last=last,
            factor=factor,
            lift=lift,
        ),
        in_specs=[whole] * len(operands),
        out_specs=tuple([whole] * len(out_shape)),
        out_shape=out_shape,
        cost_estimate=pl.CostEstimate(
            flops=4 * all_keys * parts * width * dim,
            bytes_accessed=2 * parts * width * dim * 4,
            transcendentals=all_keys * parts * width,
        ),
        compiler_params=room(32),
        name="attend",
    )(*near(*operands))


def out_kernel(place, parts, w0, w1, w2, w3, mine, other, both, held, done):
    copies = [
        pltpu.make_async_copy(w, held.at[h], done.at[h]) for h, w in enumerate((w0, w1, w2, w3))
    ]
    for copy in copies:
        copy.start()
    chips = len(copies)
    dim = parts.shape[1] - 16
    rows = mine.shape[0]
    for h, copy in enumerate(copies):
        chip = jax.lax.rem(place[0] + h, chips)
        group = [y * chips + chip for y in range(parts.shape[0] // chips)]
        tail = [parts[i, dim : dim + 16].astype(F32) for i in group]
        lse = [t[0:1] + t[1:2] + t[2:3] for t in tail]
        top = functools.reduce(jnp.maximum, lse)
        share = [jnp.exp2(v - top) for v in lse]
        whole = functools.reduce(jnp.add, share)
        merged = functools.reduce(
            jnp.add, [parts[i, 0:dim].astype(F32) * s for i, s in zip(group, share)]
        )
        turn = jnp.transpose(merged / whole)
        attended = jnp.concatenate(
            [turn[at : at + 2 * rows] for at in range(0, turn.shape[0], 2 * rows)], axis=1
        ).astype(BF16)
        copy.wait()
        partial = jnp.dot(attended, held[h], preferred_element_type=F32)
        partial = partial.astype(BF16).astype(F32)
        both[...] = partial if h == 0 else both[...] + partial
    mine[...] = both[pl.ds(pl.multiple_of(place[1] * rows, rows), rows)]
    other[...] = both[pl.ds(pl.multiple_of((1 - place[1]) * rows, rows), rows)]


def final_kernel(latent, mine, other, gate, gain, out):
    mixed = mine[...] + other[...]
    out[...] = (latent[...].astype(F32) + gate[...] * (rms_rows(mixed) * gain[...])).astype(BF16)


def body(
    latent,
    condition,
    context_condition,
    context,
    w_shift,
    w_scale,
    w_gate,
    pre_gain,
    post_gain,
    query_gain,
    key_gain,
    w_query,
    w_key,
    w_value,
    w_out,
):
    tp_count = lax.axis_size(TP)
    y_count = lax.axis_size("y")
    model = latent.shape[1]
    head_dim = query_gain.shape[0]
    tok_dev = latent.shape[0] * tp_count
    ctx_dev = context.shape[0]
    heads_dev = w_query.shape[1] // head_dim
    factor = head_dim ** (-0.5) * LOG2E
    lift = math.log(tok_dev / (4.0 * ctx_dev)) * LOG2E

    def receive(value, axis, hop):
        size = lax.axis_size(axis)
        return lax.ppermute(value, axis, [((i + hop) % size, i) for i in range(size)])

    chips = lax.axis_size("x")
    whole = pl.BlockSpec(memory_space=pltpu.VMEM)
    gains = jnp.stack([query_gain, key_gain])
    partial_mod = pl.pallas_call(
        modulation_kernel,
        in_specs=[whole] * 5,
        out_specs=whole,
        out_shape=jax.ShapeDtypeStruct((lax.axis_size("z"), 5, w_shift.shape[1]), F32),
        compiler_params=room(16),
        name="modulation",
    )(*far(condition[None], context_condition[None], w_shift, w_scale, w_gate))
    partial_mod = lax.all_to_all(partial_mod, "z", 0, 0, tiled=True)
    partial_mod = pl.pallas_call(
        spread_kernel,
        in_specs=[whole],
        out_specs=whole,
        out_shape=jax.ShapeDtypeStruct((y_count * tp_count, *partial_mod.shape[1:]), F32),
        compiler_params=room(4),
        name="spread",
    )(*near(partial_mod))
    pieces = lax.all_to_all(partial_mod, ("y", *TP), 0, 0, tiled=True)
    mine = [latent] + [receive(latent, "x", h) for h in (1, 2, 3)]
    other = jnp.concatenate(mine, axis=0)
    other = receive(other, "c", 1)

    positions = (lax.axis_index("z") * y_count + lax.axis_index("y")) * tok_dev + jnp.arange(tok_dev)
    cos, sa, sb = rotation_tables(positions, GRID_W, head_dim)
    msg_rows = 2 * tok_dev + 2 * ctx_dev
    place = jnp.stack([lax.axis_index("x"), lax.axis_index("c")]).astype(jnp.int32)
    message, normed, gate = pl.pallas_call(
        project_kernel,
        in_specs=[pl.BlockSpec(memory_space=pltpu.SMEM)] + [whole] * 14,
        out_specs=(whole, whole, whole),
        out_shape=(
            jax.ShapeDtypeStruct((msg_rows, head_dim), BF16),
            pltpu.VMEM((tok_dev, model), BF16),
            jax.ShapeDtypeStruct((1, model), F32),
        ),
        scratch_shapes=[pltpu.VMEM((tok_dev, model), BF16)],
        cost_estimate=pl.CostEstimate(
            flops=2 * tok_dev * model * 2 * head_dim,
            bytes_accessed=2 * model * (2 * head_dim + tok_dev),
            transcendentals=0,
        ),
        compiler_params=room(24),
        name="project",
    )(
        place,
        *near(
            *mine,
            other,
            pieces,
            context,
            pre_gain[None],
            w_key,
            w_value,
            gains,
            cos,
            sa,
            sb,
        ),
    )
    query = pl.pallas_call(
        functools.partial(query_kernel, chips=chips),
        in_specs=[whole] * 6,
        out_specs=whole,
        out_shape=jax.ShapeDtypeStruct((y_count, head_dim, heads_dev * tok_dev), BF16),
        cost_estimate=pl.CostEstimate(
            flops=2 * tok_dev * model * 2 * head_dim,
            bytes_accessed=2 * model * (2 * head_dim + tok_dev),
            transcendentals=0,
        ),
        compiler_params=room(16),
        name="query",
    )(*near(normed, w_query, gains, cos, sa, sb))

    far_up = receive(message, "z", 6)
    far_down = receive(message, "z", -5)
    up, down = receive(message, "z", 1), receive(message, "z", -1)
    q_all = lax.all_to_all(query, "y", 0, 0, tiled=True)
    across = receive(w_out, "x", 2)
    after = receive(w_out, "x", 1)
    before = receive(w_out, "x", 3)
    w_outs = [w_out, after, across, before]
    to_down, to_up = bundled(
        [up, far_up, far_down, down], ((0, 1, 2), (1, 2, 3)), 3 * msg_rows
    )
    ups, downs = receive(to_down, "z", 1), receive(to_up, "z", -1)
    last_ups = receive(ups, "z", 1)
    (to_up,) = bundled([downs], ((0,),), 2 * msg_rows)
    last_downs = receive(to_up, "z", -1)
    shared = (tok_dev, ctx_dev, factor, lift, chips)
    carry = attend(q_all, [message, up, down, far_up, far_down], None, False, *shared)
    carry = attend(q_all, [ups, downs], carry, False, *shared)
    (partials,) = attend(q_all, [last_ups, last_downs], carry, True, *shared)
    returned = lax.all_to_all(partials, ("y", "x"), 0, 0, tiled=True)
    rows = latent.shape[0]
    sums, others = pl.pallas_call(
        out_kernel,
        in_specs=[pl.BlockSpec(memory_space=pltpu.SMEM), whole]
        + [pl.BlockSpec(memory_space=pltpu.HBM)] * 4,
        out_specs=(whole, whole),
        out_shape=(
            jax.ShapeDtypeStruct((rows, model), F32),
            jax.ShapeDtypeStruct((rows, model), F32),
        ),
        scratch_shapes=[
            pltpu.VMEM((2 * rows, model), F32),
            pltpu.VMEM((4, *w_out.shape), BF16),
            pltpu.SemaphoreType.DMA((4,)),
        ],
        compiler_params=room(16),
        cost_estimate=pl.CostEstimate(
            flops=2 * tok_dev * model * heads_dev * head_dim,
            bytes_accessed=4 * tok_dev * model,
            transcendentals=0,
        ),
        name="out",
    )(place, *near(returned), *far(*w_outs))
    others = receive(others, "c", 1)
    return pl.pallas_call(
        final_kernel,
        in_specs=[whole] * 5,
        out_specs=whole,
        out_shape=jax.ShapeDtypeStruct((rows, model), BF16),
        compiler_params=room(16),
        name="final",
    )(*near(latent, sums, others, gate, post_gain[None]))


def solution(mesh):
    torus = Mesh(mesh.devices.reshape(16, 4, 4, 2), ALL)
    sp = ("z", "y")
    placed = (
        P(ALL, None),
        P(sp),
        P(sp),
        P(sp, None),
        P(sp, TP),
        P(sp, TP),
        P(sp, TP),
        P(),
        P(),
        P(),
        P(),
        P(None, TP),
        P(None, TP),
        P(None, TP),
        P(TP, None),
    )
    return jax.shard_map(body, mesh=torus, in_specs=placed, out_specs=P(ALL, None), check_vma=False)
```

```python
import functools
import math

import jax
import jax.numpy as jnp
from jax import lax
from jax.experimental import pallas as pl
from jax.experimental.pallas import tpu as pltpu
from jax.sharding import Mesh
from jax.sharding import PartitionSpec as P


RESIDENT = (3, 1)
FETCHED = (0, 2)
GRID_W = 64
LOG2E = math.log2(math.e)
TP = ("x", "c")
ALL = ("z", "y", *TP)
F32 = jnp.float32
BF16 = jnp.bfloat16


def room(mebibytes):
    return pltpu.CompilerParams(vmem_limit_bytes=mebibytes << 20)


def near(*arrays):
    return [pltpu.with_memory_space_constraint(a, pltpu.VMEM) for a in arrays]


def far(*arrays):
    return [pltpu.with_memory_space_constraint(a, pltpu.HBM) for a in arrays]


def rms_rows(values):
    return values * lax.rsqrt(jnp.mean(values * values, axis=-1, keepdims=True) + 1e-06)


def rotation_tables(positions, grid_width, head_dim):
    half = head_dim // 2
    quarter = head_dim // 4
    lane = jnp.arange(head_dim)
    j = (lane % quarter).astype(F32)
    freqs = 10000.0 ** (-(2.0 * j) / half)
    row_pos = (positions // grid_width).astype(F32)[:, None]
    col_pos = (positions % grid_width).astype(F32)[:, None]
    angle = jnp.where(lane[None] < half, row_pos, col_pos) * freqs[None]
    first = ((lane % half) < quarter)[None]
    sine = jnp.sin(angle)
    return (
        jnp.cos(angle),
        jnp.where(first, -sine, 0.0),
        jnp.where(first, 0.0, sine),
    )


def modulation_kernel(cond, ctx_cond, w_shift, w_scale, w_gate, out):
    both = jnp.concatenate([cond[...].astype(F32), ctx_cond[...].astype(F32)], axis=0)
    both = jax.nn.silu(both).astype(BF16)
    shift, scale, gate = (
        jnp.dot(both, w[...], preferred_element_type=F32) for w in (w_shift, w_scale, w_gate)
    )
    rows = jnp.concatenate([shift[0:1], scale[0:1], shift[1:2], scale[1:2], gate[0:1]], axis=0)
    for i in range(out.shape[0]):
        out[i] = rows


def turned(v, gain_row, cos, sa, sb):
    head_dim = v.shape[1]
    quarter = head_dim // 4
    v = rms_rows(v) * gain_row
    up = pltpu.roll(v, head_dim - quarter, 1)
    down = pltpu.roll(v, quarter, 1)
    return v * cos[...] + up * sa[...] + down * sb[...]


def project_kernel(place, *refs):
    mine, other = refs[:4], refs[4]
    pieces, ctx, gain, wk, wv, gains, cos, sa, sb, msg, normed, gate, lat = refs[5:]
    rows = lat.shape[0]
    part = mine[0].shape[0]
    for h in range(4):
        at = jax.lax.rem(place[0] + h, 4) * 2
        lat[pl.ds(pl.multiple_of((at + place[1]) * part, part), part)] = mine[h][...]
        lat[pl.ds(pl.multiple_of((at + 1 - place[1]) * part, part), part)] = other[
            h * part : (h + 1) * part
        ]
    slots = 2 * 4
    mods = jnp.concatenate(
        [
            functools.reduce(
                jnp.add, [pieces[y * slots + t] for y in range(pieces.shape[0] // slots)]
            )
            for t in range(slots)
        ],
        axis=1,
    )
    gate[...] = mods[4:5]
    ctx_rows = ctx.shape[0]
    g = gain[...]
    x = rms_rows(lat[...].astype(F32)) * g
    x = (x * (1.0 + mods[1:2]) + mods[0:1]).astype(BF16)
    normed[...] = x
    c = rms_rows(ctx[...].astype(F32)) * g
    c = (c * (1.0 + mods[3:4]) + mods[2:3]).astype(BF16)
    both = jnp.concatenate([x, c], axis=0)
    k = jnp.dot(both, wk[...], preferred_element_type=F32)
    v = jnp.dot(both, wv[...], preferred_element_type=F32)
    msg[0:rows] = turned(k[:rows], gains[1:2], cos, sa, sb).astype(BF16)
    msg[rows : 2 * rows] = v[:rows].astype(BF16)
    tail = jnp.concatenate([rms_rows(k[rows:]) * gains[1:2], v[rows:]], axis=0)
    msg[2 * rows : 2 * rows + 2 * ctx_rows] = tail.astype(BF16)


def query_kernel(normed, wq, gains, cos, sa, sb, q_out, *, chips):
    head_dim = gains.shape[1]
    q = jnp.dot(normed[...], wq[...], preferred_element_type=F32)
    heads = [
        turned(q[:, h : h + head_dim], gains[0:1], cos, sa, sb)
        for h in range(0, q.shape[1], head_dim)
    ]
    part = q.shape[0] // chips
    rows = [v[i * part : (i + 1) * part] for i in range(chips) for v in heads]
    qt = jnp.transpose(jnp.concatenate(rows, axis=0)).astype(BF16)
    for i in range(q_out.shape[0]):
        q_out[i] = qt


def spread_kernel(blocks, out):
    total = functools.reduce(jnp.add, [blocks[i] for i in range(blocks.shape[0])])
    for i in range(out.shape[0]):
        out[i] = total


def bundle_kernel(*refs, groups):
    outs = refs[-len(groups) :]
    for out, group in zip(outs, groups):
        at = 0
        for k in group:
            rows = min(refs[k].shape[0], out.shape[0] - at)
            out[at : at + rows] = refs[k][0:rows]
            at += rows


def bundled(arrays, groups, rows):
    whole = pl.BlockSpec(memory_space=pltpu.VMEM)
    return pl.pallas_call(
        functools.partial(bundle_kernel, groups=groups),
        in_specs=[whole] * len(arrays),
        out_specs=tuple([whole] * len(groups)),
        out_shape=tuple(
            jax.ShapeDtypeStruct((rows, arrays[0].shape[1]), arrays[0].dtype) for _ in groups
        ),
        compiler_params=room(4),
        name="bundle",
    )(*near(*arrays))


def attend_kernel(*refs, counts, keys, extra, first, last, factor, lift):
    refs = list(refs)
    q = refs.pop(0)
    span = 2 * (keys + extra)
    blocks = []
    for count in counts:
        ref = refs.pop(0)
        blocks += [(ref, i * span) for i in range(count)]
    if not first:
        m_in, l_in, acc_in = refs.pop(0), refs.pop(0), refs.pop(0)
    tails = [ref[at + 2 * keys : at + span].astype(F32) for ref, at in blocks]
    ctx_key = jnp.concatenate([t[:extra] for t in tails], axis=0).astype(BF16)
    ctx_value = jnp.concatenate([t[extra:] for t in tails], axis=0).astype(BF16)

    wide = 2
    width = q.shape[2]

    def both(ref, i):
        return jnp.concatenate([ref[wide * i + w] for w in range(wide)], axis=1)

    def tile(i, unused):
        qv = both(q, i)
        scores = [
            jnp.dot(ref[at : at + keys], qv, preferred_element_type=F32) for ref, at in blocks
        ]
        largest = functools.reduce(
            jnp.maximum, [jnp.max(s, axis=0, keepdims=True) for s in scores]
        )
        ctx_scores = jnp.dot(ctx_key, qv, preferred_element_type=F32) * factor + lift
        largest = jnp.maximum(largest * factor, jnp.max(ctx_scores, axis=0, keepdims=True))
        if not first:
            before = both(m_in, i)
            largest = jnp.maximum(largest, before)
        terms = jnp.exp2(ctx_scores - largest)
        total = jnp.sum(terms, axis=0, keepdims=True)
        acc = weighted(ctx_value, terms)
        if not first:
            fade = jnp.exp2(before - largest)
            total = total + both(l_in, i) * fade
            acc = acc + both(acc_in, i) * fade
        for s, (ref, at) in zip(scores, blocks):
            terms = jnp.exp2(s * factor - largest)
            total = total + jnp.sum(terms, axis=0, keepdims=True)
            acc = acc + weighted(ref[at + keys : at + 2 * keys], terms)
        if last:
            acc = acc / total
            lse = largest + jnp.log2(total)
            hi = lse.astype(BF16).astype(F32)
            mid = (lse - hi).astype(BF16).astype(F32)
            low = lse - hi - mid
            row = lax.broadcasted_iota(jnp.int32, (16, lse.shape[1]), 0)
            packed = jnp.where(
                row == 0, hi, jnp.where(row == 1, mid, jnp.where(row == 2, low, 0.0))
            )
        for w in range(wide):
            at = slice(w * width, (w + 1) * width)
            if last:
                (out,) = refs
                dim, lanes = acc.shape[0], out.shape[2]
                for n in range(width // lanes):
                    at = slice(w * width + n * lanes, w * width + (n + 1) * lanes)
                    to = (wide * i + w) * (width // lanes) + n
                    out[to, 0:dim] = acc[:, at].astype(BF16)
                    out[to, dim : dim + 16] = packed[:, at].astype(BF16)
            else:
                m_out, l_out, acc_out = refs
                m_out[wide * i + w] = largest[:, at]
                l_out[wide * i + w] = total[:, at]
                acc_out[wide * i + w] = acc[:, at]
        return unused

    lax.fori_loop(0, q.shape[0] // wide, tile, 0, unroll=True)


def weighted(values, terms):
    return lax.dot_general(
        values, terms.astype(BF16), (((0,), (0,)), ((), ())), preferred_element_type=F32
    )


def attend(q_all, bundles, carry, last, keys, extra, factor, lift, chips):
    parts, dim, width = q_all.shape
    first = carry is None
    counts = tuple(b.shape[0] // (2 * (keys + extra)) for b in bundles)
    operands = [q_all, *bundles] + ([] if first else list(carry))
    if last:
        out_shape = (jax.ShapeDtypeStruct((parts * chips, dim + 16, width // chips), BF16),)
    else:
        out_shape = (
            pltpu.VMEM((parts, 1, width), F32),
            pltpu.VMEM((parts, 1, width), F32),
            pltpu.VMEM((parts, dim, width), F32),
        )
    whole = pl.BlockSpec(memory_space=pltpu.VMEM)
    all_keys = (keys + extra) * sum(counts)
    return pl.pallas_call(
        functools.partial(
            attend_kernel,
            counts=counts,
            keys=keys,
            extra=extra,
            first=first,
            last=last,
            factor=factor,
            lift=lift,
        ),
        in_specs=[whole] * len(operands),
        out_specs=tuple([whole] * len(out_shape)),
        out_shape=out_shape,
        cost_estimate=pl.CostEstimate(
            flops=4 * all_keys * parts * width * dim,
            bytes_accessed=2 * parts * width * dim * 4,
            transcendentals=all_keys * parts * width,
        ),
        compiler_params=room(32),
        name="attend",
    )(*near(*operands))


def out_kernel(place, parts, w0, w1, w2, w3, mine, other, both, held, done):
    weights = (w0, w1, w2, w3)
    copies = {
        h: pltpu.make_async_copy(weights[h], held.at[n], done.at[n]) for n, h in enumerate(FETCHED)
    }
    for copy in copies.values():
        copy.start()
    chips = len(weights)
    dim = parts.shape[1] - 16
    rows = mine.shape[0]
    for h in (*RESIDENT, *FETCHED):
        chip = jax.lax.rem(place[0] + h, chips)
        group = [y * chips + chip for y in range(parts.shape[0] // chips)]
        tail = [parts[i, dim : dim + 16].astype(F32) for i in group]
        lse = [t[0:1] + t[1:2] + t[2:3] for t in tail]
        top = functools.reduce(jnp.maximum, lse)
        share = [jnp.exp2(v - top) for v in lse]
        whole = functools.reduce(jnp.add, share)
        merged = functools.reduce(
            jnp.add, [parts[i, 0:dim].astype(F32) * s for i, s in zip(group, share)]
        )
        turn = jnp.transpose(merged / whole)
        attended = jnp.concatenate(
            [turn[at : at + 2 * rows] for at in range(0, turn.shape[0], 2 * rows)], axis=1
        ).astype(BF16)
        if h in copies:
            copies[h].wait()
        rows_out = held[FETCHED.index(h)] if h in copies else weights[h][...]
        partial = jnp.dot(attended, rows_out, preferred_element_type=F32)
        partial = partial.astype(BF16).astype(F32)
        both[...] = partial if h == (*RESIDENT, *FETCHED)[0] else both[...] + partial
    mine[...] = both[pl.ds(pl.multiple_of(place[1] * rows, rows), rows)]
    other[...] = both[pl.ds(pl.multiple_of((1 - place[1]) * rows, rows), rows)]


def final_kernel(latent, mine, other, gate, gain, out):
    mixed = mine[...] + other[...]
    out[...] = (latent[...].astype(F32) + gate[...] * (rms_rows(mixed) * gain[...])).astype(BF16)


def body(
    latent,
    condition,
    context_condition,
    context,
    w_shift,
    w_scale,
    w_gate,
    pre_gain,
    post_gain,
    query_gain,
    key_gain,
    w_query,
    w_key,
    w_value,
    w_out,
):
    tp_count = lax.axis_size(TP)
    y_count = lax.axis_size("y")
    model = latent.shape[1]
    head_dim = query_gain.shape[0]
    tok_dev = latent.shape[0] * tp_count
    ctx_dev = context.shape[0]
    heads_dev = w_query.shape[1] // head_dim
    factor = head_dim ** (-0.5) * LOG2E
    lift = math.log(tok_dev / (4.0 * ctx_dev)) * LOG2E

    def receive(value, axis, hop):
        size = lax.axis_size(axis)
        return lax.ppermute(value, axis, [((i + hop) % size, i) for i in range(size)])

    chips = lax.axis_size("x")
    whole = pl.BlockSpec(memory_space=pltpu.VMEM)
    gains = jnp.stack([query_gain, key_gain])
    partial_mod = pl.pallas_call(
        modulation_kernel,
        in_specs=[whole] * 5,
        out_specs=whole,
        out_shape=jax.ShapeDtypeStruct((lax.axis_size("z"), 5, w_shift.shape[1]), F32),
        compiler_params=room(16),
        name="modulation",
    )(*far(condition[None], context_condition[None], w_shift, w_scale, w_gate))
    partial_mod = lax.all_to_all(partial_mod, "z", 0, 0, tiled=True)
    partial_mod = pl.pallas_call(
        spread_kernel,
        in_specs=[whole],
        out_specs=whole,
        out_shape=jax.ShapeDtypeStruct((y_count * tp_count, *partial_mod.shape[1:]), F32),
        compiler_params=room(4),
        name="spread",
    )(*near(partial_mod))
    pieces = lax.all_to_all(partial_mod, ("y", *TP), 0, 0, tiled=True)
    mine = [latent] + [receive(latent, "x", h) for h in (1, 2, 3)]
    other = jnp.concatenate(mine, axis=0)
    other = receive(other, "c", 1)

    positions = (lax.axis_index("z") * y_count + lax.axis_index("y")) * tok_dev + jnp.arange(tok_dev)
    cos, sa, sb = rotation_tables(positions, GRID_W, head_dim)
    msg_rows = 2 * tok_dev + 2 * ctx_dev
    place = jnp.stack([lax.axis_index("x"), lax.axis_index("c")]).astype(jnp.int32)
    message, normed, gate = pl.pallas_call(
        project_kernel,
        in_specs=[pl.BlockSpec(memory_space=pltpu.SMEM)] + [whole] * 14,
        out_specs=(whole, whole, whole),
        out_shape=(
            jax.ShapeDtypeStruct((msg_rows, head_dim), BF16),
            pltpu.VMEM((tok_dev, model), BF16),
            jax.ShapeDtypeStruct((1, model), F32),
        ),
        scratch_shapes=[pltpu.VMEM((tok_dev, model), BF16)],
        cost_estimate=pl.CostEstimate(
            flops=2 * tok_dev * model * 2 * head_dim,
            bytes_accessed=2 * model * (2 * head_dim + tok_dev),
            transcendentals=0,
        ),
        compiler_params=room(24),
        name="project",
    )(
        place,
        *near(
            *mine,
            other,
            pieces,
            context,
            pre_gain[None],
            w_key,
            w_value,
            gains,
            cos,
            sa,
            sb,
        ),
    )
    query = pl.pallas_call(
        functools.partial(query_kernel, chips=chips),
        in_specs=[whole] * 6,
        out_specs=whole,
        out_shape=jax.ShapeDtypeStruct((y_count, head_dim, heads_dev * tok_dev), BF16),
        cost_estimate=pl.CostEstimate(
            flops=2 * tok_dev * model * 2 * head_dim,
            bytes_accessed=2 * model * (2 * head_dim + tok_dev),
            transcendentals=0,
        ),
        compiler_params=room(16),
        name="query",
    )(*near(normed, w_query, gains, cos, sa, sb))

    far_up = receive(message, "z", 6)
    far_down = receive(message, "z", -5)
    up, down = receive(message, "z", 1), receive(message, "z", -1)
    q_all = lax.all_to_all(query, "y", 0, 0, tiled=True)
    across = receive(w_out, "x", 2)
    after = receive(w_out, "x", 1)
    before = receive(w_out, "x", 3)
    w_outs = [w_out, after, across, before]
    to_down, to_up = bundled(
        [up, far_up, far_down, down], ((0, 1, 2), (1, 2, 3)), 3 * msg_rows
    )
    ups, downs = receive(to_down, "z", 1), receive(to_up, "z", -1)
    last_ups = receive(ups, "z", 1)
    (to_up,) = bundled([downs], ((0,),), 2 * msg_rows)
    last_downs = receive(to_up, "z", -1)
    shared = (tok_dev, ctx_dev, factor, lift, chips)
    carry = attend(q_all, [message, up, down, far_up, far_down], None, False, *shared)
    carry = attend(q_all, [ups, downs], carry, False, *shared)
    (partials,) = attend(q_all, [last_ups, last_downs], carry, True, *shared)
    returned = lax.all_to_all(partials, ("y", "x"), 0, 0, tiled=True)
    rows = latent.shape[0]
    sums, others = pl.pallas_call(
        out_kernel,
        in_specs=[pl.BlockSpec(memory_space=pltpu.SMEM), whole]
        + [whole if h in RESIDENT else pl.BlockSpec(memory_space=pltpu.HBM) for h in range(4)],
        out_specs=(whole, whole),
        out_shape=(
            jax.ShapeDtypeStruct((rows, model), F32),
            jax.ShapeDtypeStruct((rows, model), F32),
        ),
        scratch_shapes=[
            pltpu.VMEM((2 * rows, model), F32),
            pltpu.VMEM((len(FETCHED), *w_out.shape), BF16),
            pltpu.SemaphoreType.DMA((len(FETCHED),)),
        ],
        compiler_params=room(16),
        cost_estimate=pl.CostEstimate(
            flops=2 * tok_dev * model * heads_dev * head_dim,
            bytes_accessed=4 * tok_dev * model,
            transcendentals=0,
        ),
        name="out",
    )(place, *near(returned), *[(near if h in RESIDENT else far)(w)[0] for h, w in enumerate(w_outs)])
    others = receive(others, "c", 1)
    return pl.pallas_call(
        final_kernel,
        in_specs=[whole] * 5,
        out_specs=whole,
        out_shape=jax.ShapeDtypeStruct((rows, model), BF16),
        compiler_params=room(16),
        name="final",
    )(*near(latent, sums, others, gate, post_gain[None]))


def solution(mesh):
    torus = Mesh(mesh.devices.reshape(16, 4, 4, 2), ALL)
    sp = ("z", "y")
    placed = (
        P(ALL, None),
        P(sp),
        P(sp),
        P(sp, None),
        P(sp, TP),
        P(sp, TP),
        P(sp, TP),
        P(),
        P(),
        P(),
        P(),
        P(None, TP),
        P(None, TP),
        P(None, TP),
        P(TP, None),
    )
    return jax.shard_map(body, mesh=torus, in_specs=placed, out_specs=P(ALL, None), check_vma=False)
```
